32 devices in a mesh: gr: 2 (over x), sp: 4 (over z), tp: 4 (over y, core).
Axes of the slice: x: 2, y: 2, z: 4, core: 2. Of those that a mesh axis runs over, the one named last changes fastest.
Arguments:
- tokens: bfloat16 [8, 8192, 2048], P('gr', ('sp', 'tp')), parts along dimension 0, may hold values from -6 to 6
- norm_gain: float32 [2048], replicated, may hold values from 0.1 to 1.9
- w_key: bfloat16 [2048, 256], replicated, may hold values from -0.125 to 0.125
- w_value: bfloat16 [2048, 256], replicated, may hold values from -0.125 to 0.125
- new_query: bfloat16 [8, 32, 64], P('gr'), parts along dimension 0, may hold values from -360 to 360
- cum_gate: float32 [8, 4, 8192], P(('gr', 'sp'), 'tp'), parts along dimension 0, may hold values from -1025 to 0, as said below
Outputs:
- kv_cache: bfloat16 [8, 4, 8192, 128], P(('gr', 'sp'), 'tp'), parts along dimension 0
- first_read: float32 [8, 32, 64], P('gr'), parts along dimension 0
The draws below stay inside these ranges and needn't reach their ends.
There are 2 independent parts, one for each index of `gr`. The reference program is written for one: setup_inputs(seed, part) draws one part's arguments, and reference() takes and returns one part's arrays. A program takes and returns all parts, laid end to end along the dimension named above; an argument that names none is the same for every part. Nothing has to cross between parts.
Inputs may be any that keep to these rules, and one draw needn't show every extreme that they name: `cum_gate`: for each sequence and key head, the running sum along the positions of the sequence of negative log forget gates; it never rises from one position to the next.
All inputs are finite; a program needn't handle non-finite values.
Results may differ from the reference program's by a relative error of at most 0.0014.
The reference program's roundings to bfloat16 on the way (of `normed`, `keys_all` and `values_all`) count: a program that leaves them out, or rounds other values in their place, can miss the bound.
Values may be sent and summed in bfloat16 or wider, within the bound.
No kernel may reach another device: no remote copies, remote signals or barrier semaphores. Data moves between devices by JAX's collectives and lax.ppermute only.
A program may use at most 64 MiB of HBM per device.

```python
from functools import partial
import jax
import jax.numpy as jnp
from jax import lax

D = 2048
HD = 64
QH = 32
KVH = 4
SEQS = 4
POS_DEV = 512
BLOCKS = 16
LEN = 8192
CLASSES = 1
HALVES = 1
PIECE = 512


def draw_new_query(key, part):
    base = 3.0 * jax.random.normal(jax.random.fold_in(key, 3), (SEQS, QH, HD), jnp.float32)
    base = jnp.clip(base, -18.0, 18.0)
    return base.astype(jnp.bfloat16)


def draw_cum_gate(key, part):
    flag_key = jax.random.fold_in(key, 11)
    fast_flags = jax.random.randint(flag_key, (SEQS, KVH, 1, 1), 0, 2) == 1
    fast_rate = jnp.exp(jax.random.uniform(jax.random.fold_in(key, 12), (SEQS, KVH, 1, 1), jnp.float32, jnp.log(0.01), jnp.log(1.0 / 30.0)))
    slow_rate = jnp.exp(jax.random.uniform(jax.random.fold_in(key, 13), (SEQS, KVH, 1, 1), jnp.float32, jnp.log(0.3), jnp.log(1.0))) / LEN
    base_rate = jnp.where(fast_flags, fast_rate, slow_rate)
    block_factor = jnp.exp(jax.random.uniform(jax.random.fold_in(key, 14), (SEQS, KVH, BLOCKS, 1), jnp.float32, jnp.log(0.5), jnp.log(2.0)))
    jitter = jax.random.uniform(jax.random.fold_in(key, 15), (SEQS, KVH, BLOCKS, POS_DEV), jnp.float32, 0.25, 1.75)
    log_gate = -(base_rate * block_factor * jitter)
    running = jnp.cumsum(log_gate.reshape(SEQS, KVH, LEN), axis=-1)
    laid = running.reshape(SEQS, KVH, BLOCKS, CLASSES, HALVES, PIECE).transpose(0, 3, 1, 4, 2, 5)
    return laid.reshape(SEQS * CLASSES, KVH * HALVES, BLOCKS * PIECE)


def block_levels(key, dims, cuts, least, high):
    loudness = 1.0
    for dim, parts in cuts:
        heights = jax.random.uniform(jax.random.fold_in(jax.random.fold_in(key, 6), dim), (parts,), jnp.float32, least / len(cuts), high / len(cuts))
        loudness = loudness * jnp.repeat(jnp.exp(heights), dims[dim] // parts).reshape((-1,) + (1,) * (len(dims) - 1 - dim))
    return loudness


def bell_draw(rng, shape, deviation, reach, split=(), kind=jnp.bfloat16):
    factor_of = block_levels(rng, shape, split, -0.22, 0.18) if split else 1.0
    values = jax.random.normal(rng, shape, jnp.float32) * deviation * factor_of
    return jnp.minimum(jnp.maximum(values, -reach), reach).astype(kind)


def setup_inputs(seed: int = 0, part: int = 0) -> dict:
    key_of = jax.random.split(jax.random.key(seed), 7)
    part_splits = jax.random.split(jax.random.fold_in(key_of[6], part), 7)
    return {
        "tokens": bell_draw(part_splits[0], (SEQS, LEN, D), 1.0, 6.0, ((1, 16),)),
        "norm_gain": jnp.clip(1.0 + 0.18 * jax.random.normal(key_of[1], (D,), jnp.float32), 0.1, 1.9),
        "w_key": bell_draw(key_of[2], (D, KVH * HD), D ** -0.5, 0.125),
        "w_value": bell_draw(key_of[3], (D, KVH * HD), D ** -0.5, 0.125),
        "new_query": draw_new_query(jax.random.fold_in(jax.random.fold_in(key_of[6], part), 71), part),
        "cum_gate": draw_cum_gate(jax.random.fold_in(jax.random.fold_in(key_of[6], part), 71), part),
    }


NORM_FLOOR = 0.05

def project_block(norm_gain, w_key, w_value, pos_block):
    widened = pos_block.astype(jnp.float32)
    inverse_rms = lax.rsqrt(lax.optimization_barrier(jnp.mean(widened * widened, axis=-1, keepdims=True)) + NORM_FLOOR)
    normed = (widened * inverse_rms * norm_gain.astype(jnp.float32)).astype(jnp.bfloat16)
    keys_made = jnp.dot(normed, w_key, preferred_element_type=jnp.float32).astype(jnp.bfloat16)
    values_made = jnp.dot(normed, w_value, preferred_element_type=jnp.float32).astype(jnp.bfloat16)
    keys_made = keys_made.reshape(POS_DEV, KVH, HD)
    values_made = values_made.reshape(POS_DEV, KVH, HD)
    return jnp.concatenate([keys_made, values_made], axis=-1)

def reference(tokens, norm_gain, w_key, w_value, new_query, cum_gate):
    pos_blocks = tokens.reshape(SEQS * BLOCKS, POS_DEV, D)
    stacked = lax.map(partial(project_block, norm_gain, w_key, w_value), pos_blocks)
    stacked = stacked.reshape(SEQS, BLOCKS, CLASSES, HALVES, PIECE, KVH, 2 * HD)
    kv_cache = stacked.transpose(0, 2, 5, 3, 1, 4, 6).reshape(SEQS * CLASSES, KVH * HALVES, BLOCKS * PIECE, 2 * HD)
    per_head = kv_cache.reshape(SEQS, CLASSES, KVH, HALVES, BLOCKS * PIECE, 2 * HD)
    per_head = per_head.transpose(0, 2, 1, 3, 4, 5).reshape(SEQS, KVH, LEN, 2 * HD)
    gates = cum_gate.reshape(SEQS, CLASSES, KVH, HALVES, BLOCKS * PIECE)
    gates = gates.transpose(0, 2, 1, 3, 4).reshape(SEQS, KVH, LEN)
    keys_all = per_head[..., :HD].astype(jnp.float32)
    values_all = per_head[..., HD:].astype(jnp.float32)
    grouped = new_query.astype(jnp.float32).reshape(SEQS, KVH, QH // KVH, HD)
    scores = jnp.einsum('sgqd,sgpd->sgqp', grouped, keys_all, precision=lax.Precision.HIGHEST)
    scores = scores * HD ** (-0.5) - gates[:, :, None, :]
    row_top = lax.optimization_barrier(jnp.max(scores, axis=-1, keepdims=True))
    weights = jnp.exp(scores - row_top)
    row_total = lax.optimization_barrier(jnp.sum(weights, axis=-1))
    summed = jnp.einsum('sgqp,sgpd->sgqd', weights, values_all, precision=lax.Precision.HIGHEST)
    first_read = (summed / row_total[..., None]).reshape(SEQS, QH, HD)
    return (kv_cache, first_read)
```

```python
import functools

import jax
import jax.numpy as jnp
from jax import lax
from jax.experimental import pallas as pl
from jax.experimental.pallas import tpu as pltpu
from jax.sharding import PartitionSpec as P

HD = 64
NORM_FLOOR = 0.05
F32 = jnp.float32
BF16 = jnp.bfloat16


def divisor_up_to(total, limit):
    size = min(total, limit)
    while total % size:
        size -= 1
    return size


def project_kernel(heads, tokens_ref, gain_ref, key_ref, value_ref, out_ref):
    widened = tokens_ref[0].astype(F32)
    mean_square = jnp.mean(widened * widened, axis=-1, keepdims=True)
    normed = (widened * lax.rsqrt(mean_square + NORM_FLOOR) * gain_ref[...]).astype(BF16)
    keys = jnp.dot(normed, key_ref[...], preferred_element_type=F32)
    values = jnp.dot(normed, value_ref[...], preferred_element_type=F32)
    for head in range(heads):
        columns = slice(head * HD, (head + 1) * HD)
        both = jnp.concatenate([keys[:, columns], values[:, columns]], axis=-1)
        out_ref[0, head] = both.astype(BF16)


def project(tokens, norm_gain, w_key, w_value):
    seqs, positions, width = tokens.shape
    heads = w_key.shape[1] // HD
    tile = divisor_up_to(positions, 128)
    return pl.pallas_call(
        functools.partial(project_kernel, heads),
        grid=(seqs, positions // tile),
        in_specs=[
            pl.BlockSpec((1, tile, width), lambda s, i: (s, i, 0)),
            pl.BlockSpec((1, width), lambda s, i: (0, 0)),
            pl.BlockSpec(w_key.shape, lambda s, i: (0, 0)),
            pl.BlockSpec(w_value.shape, lambda s, i: (0, 0)),
        ],
        out_specs=pl.BlockSpec((1, heads, tile, 2 * HD), lambda s, i: (s, 0, i, 0)),
        out_shape=jax.ShapeDtypeStruct((seqs, heads, positions, 2 * HD), BF16),
        name="project",
    )(tokens, norm_gain.reshape(1, width), w_key, w_value)


def three_parts(value):
    high = value.astype(BF16)
    rest = value - high.astype(F32)
    middle = rest.astype(BF16)
    low = (rest - middle.astype(F32)).astype(BF16)
    return jnp.concatenate([high, middle, low], axis=0)


def read_kernel(chunks, query_ref, cache_ref, gate_ref, out_ref):
    rows = query_ref.shape[0]
    size = cache_ref.shape[0] // chunks
    tops, totals, sums = [], [], []
    for c in range(chunks):
        block = cache_ref[c * size : (c + 1) * size, :]
        scores = lax.dot_general(
            query_ref[...], block, (((1,), (1,)), ((), ())), preferred_element_type=F32
        )
        scores = scores * HD ** (-0.5) - gate_ref[:, c * size : (c + 1) * size]
        top = jnp.max(scores, axis=1, keepdims=True)
        weights = jnp.exp(scores - top)
        parts = jnp.dot(three_parts(weights), block, preferred_element_type=F32)
        tops.append(top)
        totals.append(jnp.sum(weights, axis=1, keepdims=True))
        sums.append(parts[:rows] + parts[rows : 2 * rows] + parts[2 * rows :])
    best = functools.reduce(jnp.maximum, tops)
    factors = [jnp.exp(top - best) for top in tops]
    summed = sum(s * f for s, f in zip(sums, factors))
    total = sum(t * f for t, f in zip(totals, factors))
    lane = lax.broadcasted_iota(jnp.int32, summed.shape, 1)
    out_ref[...] = jnp.where(lane >= HD, summed, jnp.where(lane == 0, best, total))


def read(queries, cache, gates):
    rows = queries.shape[0]
    padded = jnp.concatenate([queries, jnp.zeros_like(queries)], axis=-1)
    chunks = 4
    while cache.shape[0] % chunks:
        chunks -= 1
    return pl.pallas_call(
        functools.partial(read_kernel, chunks),
        out_shape=jax.ShapeDtypeStruct((rows, 2 * HD), F32),
        name="read",
    )(padded, cache, gates)


def gathered(tile, axis, size):
    stacked = tile[None]
    if size & (size - 1):
        return lax.all_gather(tile, axis)
    step = 1
    index = lax.axis_index(axis)
    while step < size:
        other = lax.ppermute(stacked, axis, [(i, i ^ step) for i in range(size)])
        low = (index & step) == 0
        first = jnp.where(low, stacked, other)
        second = jnp.where(low, other, stacked)
        stacked = jnp.concatenate([first, second], axis=0)
        step *= 2
    return stacked


def shards(tokens, norm_gain, w_key, w_value, new_query, cum_gate):
    seqs, positions, width = tokens.shape
    sp_count, tp_count = lax.axis_size("sp"), lax.axis_size("tp")
    heads = w_key.shape[1] // HD
    classes, halves = sp_count // seqs, tp_count // heads
    piece = positions // (classes * halves)
    devices = sp_count * tp_count
    made = project(tokens, norm_gain, w_key, w_value)
    if classes * halves > 1:
        made = made.reshape(seqs, heads, classes, halves, piece, 2 * HD)
        made = made.transpose(0, 2, 1, 3, 4, 5)
    arrived = lax.all_to_all(
        made.reshape(devices, piece, 2 * HD), ("sp", "tp"), split_axis=0, concat_axis=0, tiled=True
    )
    kv_cache = arrived.reshape(devices * piece, 2 * HD)
    query_heads = new_query.shape[1]
    group = query_heads // heads
    seq_index = lax.axis_index("sp") // classes
    head_index = lax.axis_index("tp") // halves
    queries = lax.dynamic_slice(new_query, (seq_index, head_index * group, 0), (1, group, HD))[0]
    partial_read = read(queries, kv_cache, cum_gate[0])
    tiles = gathered(gathered(partial_read, "tp", tp_count), "sp", sp_count)
    tiles = tiles.reshape(seqs, classes, heads, halves, group, 2 * HD)
    tops = tiles[..., :1]
    factors = jnp.exp(tops - jnp.max(tops, axis=(1, 3), keepdims=True))
    merged = jnp.sum(tiles * factors, axis=(1, 3))
    first_read = merged[..., HD:] / merged[..., 1:2]
    return kv_cache[None, None], first_read.reshape(seqs, query_heads, HD)


def solution(mesh):
    in_specs = (
        P("gr", ("sp", "tp"), None),
        P(),
        P(),
        P(),
        P("gr", None, None),
        P(("gr", "sp"), "tp", None),
    )
    out_specs = (P(("gr", "sp"), "tp", None, None), P("gr", None, None))
    return jax.shard_map(shards, mesh=mesh, in_specs=in_specs, out_specs=out_specs, check_vma=False)
```

```python
import functools

import jax
import jax.numpy as jnp
from jax import lax
from jax.experimental import pallas as pl
from jax.experimental.pallas import tpu as pltpu
from jax.sharding import PartitionSpec as P

HD = 64
LANES = 128
NORM_FLOOR = 0.05
F32 = jnp.float32
BF16 = jnp.bfloat16


def divisor_up_to(total, limit):
    size = min(total, limit)
    while total % size:
        size -= 1
    return size


def normalize(tokens, gain):
    widened = tokens.astype(F32)
    mean_square = jnp.mean(widened * widened, axis=-1, keepdims=True)
    return (widened * lax.rsqrt(mean_square + NORM_FLOOR) * gain).astype(BF16)


def keys_and_values(normed, key_ref, value_ref):
    keys = jnp.dot(normed, key_ref[...], preferred_element_type=F32)
    values = jnp.dot(normed, value_ref[...], preferred_element_type=F32)
    for head in range(key_ref.shape[1] // HD):
        columns = slice(head * HD, (head + 1) * HD)
        yield head, jnp.concatenate([keys[:, columns], values[:, columns]], axis=-1).astype(BF16)


def three_parts(value, axis=0):
    high = value.astype(BF16)
    rest = value - high.astype(F32)
    middle = rest.astype(BF16)
    low = (rest - middle.astype(F32)).astype(BF16)
    return jnp.concatenate([high, middle, low], axis=axis)


def project_kernel(tokens_ref, gain_ref, key_ref, value_ref, out_ref):
    normed = normalize(tokens_ref[0], gain_ref[...])
    for head, both in keys_and_values(normed, key_ref, value_ref):
        out_ref[0, head] = both


def project(tokens, norm_gain, w_key, w_value):
    seqs, positions, width = tokens.shape
    heads = w_key.shape[1] // HD
    tile = divisor_up_to(positions, 512)
    return pl.pallas_call(
        project_kernel,
        grid=(seqs, positions // tile),
        in_specs=[
            pl.BlockSpec((1, tile, width), lambda s, i: (s, i, 0)),
            pl.BlockSpec((1, width), lambda s, i: (0, 0)),
            pl.BlockSpec(w_key.shape, lambda s, i: (0, 0)),
            pl.BlockSpec(w_value.shape, lambda s, i: (0, 0)),
        ],
        out_specs=pl.BlockSpec((1, heads, tile, 2 * HD), lambda s, i: (s, 0, i, 0)),
        out_shape=jax.ShapeDtypeStruct((seqs, heads, positions, 2 * HD), BF16),
        name="project",
    )(tokens, norm_gain, w_key, w_value)


def softmax_part(query, block, gate):
    rows = query.shape[0]
    scores = lax.dot_general(query, block, (((1,), (1,)), ((), ())), preferred_element_type=F32)
    scores = scores * HD ** (-0.5) - gate
    top = jnp.max(scores, axis=1, keepdims=True)
    weights = jnp.exp(scores - top)
    parts = jnp.dot(three_parts(weights), block, preferred_element_type=F32)
    summed = parts[:rows] + parts[rows : 2 * rows] + parts[2 * rows :]
    return summed, top, jnp.sum(weights, axis=1, keepdims=True)


def packed(summed, top, total):
    lane = lax.broadcasted_iota(jnp.int32, summed.shape, summed.ndim - 1)
    return jnp.where(lane >= HD, summed, jnp.where(lane == 0, top, total))


def merged(tiles):
    best = functools.reduce(jnp.maximum, [tile[..., :1] for tile in tiles])
    factors = [jnp.exp(tile[..., :1] - best) for tile in tiles]
    both = sum(tile * factor for tile, factor in zip(tiles, factors))
    return both, best


def read_kernel(chunks, query_ref, cache_ref, gate_ref, out_ref):
    size = cache_ref.shape[0] // chunks
    tiles = []
    for c in range(chunks):
        rows = slice(c * size, (c + 1) * size)
        tiles.append(packed(*softmax_part(query_ref[...], cache_ref[rows, :], gate_ref[:, rows])))
    both, best = merged(tiles)
    out_ref[...] = packed(both, best, both[:, 1:2])


def read(queries, cache, gates):
    padded = jnp.concatenate([queries, jnp.zeros_like(queries)], axis=-1)
    chunks = 4
    while cache.shape[0] % chunks:
        chunks -= 1
    return pl.pallas_call(
        functools.partial(read_kernel, chunks),
        out_shape=jax.ShapeDtypeStruct((queries.shape[0], 2 * HD), F32),
        name="read",
    )(padded, cache, gates)


def read_after(sp_axes, tokens, norm_gain, w_key, w_value, new_query, cum_gate):
    seqs, positions, _ = tokens.shape
    sp_count, tp_count = lax.axis_size(sp_axes), lax.axis_size("tp")
    everyone = (sp_axes if isinstance(sp_axes, tuple) else (sp_axes,)) + ("tp",)
    heads = w_key.shape[1] // HD
    classes, halves = sp_count // seqs, tp_count // heads
    piece = positions // (classes * halves)
    devices = sp_count * tp_count
    made = project(tokens, norm_gain, w_key, w_value)
    made = made.reshape(seqs, heads, classes, halves, piece, 2 * HD).transpose(0, 2, 1, 3, 4, 5)
    arrived = lax.all_to_all(
        made.reshape(devices, piece, 2 * HD), everyone, split_axis=0, concat_axis=0, tiled=True
    )
    kv_cache = arrived.reshape(devices * piece, 2 * HD)
    query_heads = new_query.shape[1]
    group = query_heads // heads
    seq_index = lax.axis_index(sp_axes) // classes
    head_index = lax.axis_index("tp") // halves
    queries = lax.dynamic_slice(new_query, (seq_index, head_index * group, 0), (1, group, HD))[0]
    tile = read(queries, kv_cache, cum_gate[0])
    tiles = lax.all_gather(tile, everyone)
    tiles = tiles.reshape(seqs, classes, heads, halves, group, 2 * HD)
    tops = tiles[..., :1]
    factors = jnp.exp(tops - jnp.max(tops, axis=(1, 3), keepdims=True))
    both = jnp.sum(tiles * factors, axis=(1, 3))
    first_read = both[..., HD:] / both[..., 1:2]
    return kv_cache[None, None], first_read.reshape(seqs, query_heads, HD)


def heads_made(normed, key_ref, value_ref):
    return [both for _, both in keys_and_values(normed, key_ref, value_ref)]


def across_kernel(axes, flip, tokens_ref, gain_ref, key_hbm, value_hbm, *refs):
    out_refs, (token_ref, key_ref, value_ref, made_ref, semaphores) = refs[:-5], refs[-5:]
    upper, lower, column = (lax.axis_index(axis) for axis in axes)
    seq = (upper * lax.axis_size(axes[1]) + lower) ^ flip
    pieces, rows = token_ref.shape[:2]
    loads = [(tokens_ref.at[seq, pl.ds(i * rows, rows)], token_ref.at[i]) for i in range(pieces)]
    loads[1:1] = [(key_hbm, key_ref), (value_hbm, value_ref)]
    copies = [
        pltpu.make_async_copy(source, target, semaphores.at[i])
        for i, (source, target) in enumerate(loads)
    ]
    for copy in copies:
        copy.start()
    for i in range(pieces):
        copies[0 if i == 0 else i + 2].wait()
        normed = normalize(token_ref[i], gain_ref[...])
        if i == 0:
            copies[1].wait()
            copies[2].wait()
        for head, both in enumerate(heads_made(normed, key_ref, value_ref)):
            made_ref[head, i * rows : (i + 1) * rows] = both
    for j, out_ref in enumerate(out_refs):
        out_ref[...] = made_ref[column ^ j]


def make_across(axes, flip, tokens, norm_gain, w_key, w_value):
    _, positions, width = tokens.shape
    heads = w_key.shape[1] // HD
    pieces = 2
    anywhere, vmem = pl.BlockSpec(memory_space=pl.ANY), pl.BlockSpec(memory_space=pltpu.VMEM)
    return pl.pallas_call(
        functools.partial(across_kernel, axes, flip),
        in_specs=[anywhere, vmem, anywhere, anywhere],
        out_specs=[vmem] * heads,
        out_shape=[jax.ShapeDtypeStruct((positions, 2 * HD), BF16)] * heads,
        scratch_shapes=[
            pltpu.VMEM((pieces, positions // pieces, width), BF16),
            pltpu.VMEM(w_key.shape, BF16),
            pltpu.VMEM(w_value.shape, BF16),
            pltpu.VMEM((heads, positions, 2 * HD), BF16),
            pltpu.SemaphoreType.DMA((pieces + 2,)),
        ],
        name="across",
    )(tokens, norm_gain, w_key, w_value)


def planes(axes):
    upper, lower, column = (lax.axis_index(axis) for axis in axes)
    half = lax.axis_size(axes[1])
    return upper * half + lower, upper * half, column, half


def read_sequence(slots, blocks, query_ref, gate_ref, tile_ref):
    heads, group = len(blocks), query_ref.shape[1]
    lanes, queries, gates = 2 * HD, [], []
    for head, slot in enumerate(slots):
        query = query_ref[slot].astype(F32)
        pieces = [jnp.zeros((group, size), F32) for size in (head * lanes, (heads - head) * lanes - HD)]
        pieces.insert(1, query)
        queries.append(jnp.concatenate([piece for piece in pieces if piece.shape[1]], axis=1))
        lines = gate_ref[slot]
        gate = jnp.concatenate([lines[i : i + 1] for i in range(lines.shape[0])], axis=1)
        gates.append(jnp.broadcast_to(gate, (group, gate.shape[1])))
    query = jnp.concatenate(queries, axis=0).astype(BF16)
    block = jnp.concatenate(blocks, axis=1)
    summed, top, total = softmax_part(query, block, jnp.concatenate(gates, axis=0))
    for head, slot in enumerate(slots):
        rows = slice(head * group, (head + 1) * group)
        columns = slice(head * lanes, (head + 1) * lanes)
        tile_ref[slot] = packed(summed[rows, columns], top[rows], total[rows])


def rest_kernel(axes, heads, tokens_ref, gain_ref, key_ref, value_ref, query_ref, gate_ref, *refs):
    first_refs, refs = refs[:heads], refs[heads:]
    second_refs, (near_ref, tile_ref, _, made_ref) = refs[:heads], refs[heads:]
    step = pl.program_id(0)
    plane, near_first, column, half = planes(axes)
    made = heads_made(normalize(tokens_ref[0], gain_ref[...]), key_ref, value_ref)
    seq = jnp.where(step == 0, plane ^ (half + 1), near_first + step - 1)
    slots = [seq * heads + head for head in range(heads)]
    read_sequence(slots, made, query_ref, gate_ref, tile_ref)

    @pl.when(step == 0)
    def _():
        for head, both in enumerate(made):
            made_ref[head] = both
        for j in range(heads):
            second_refs[j][...] = made_ref[column ^ j]
        slots = [(plane ^ half) * heads + (column ^ j) for j in range(heads)]
        read_sequence(slots, [ref[...] for ref in first_refs], query_ref, gate_ref, tile_ref)

    @pl.when(step > 0)
    def _():
        for head, both in enumerate(made):
            near_ref[0, head] = both


def make_rest(axes, tokens, norm_gain, w_key, w_value, queries, gates, first):
    seqs, positions, width = tokens.shape
    heads = w_key.shape[1] // HD
    near = seqs // 2
    fixed = lambda rank: lambda i: (0,) * rank
    tile_shape = queries.shape[:2] + (2 * HD,)

    def sequence(i):
        plane, near_first, _, half = planes(axes)
        return jnp.where(i == 0, plane ^ (half + 1), near_first + i - 1), 0, 0

    made = pl.pallas_call(
        functools.partial(rest_kernel, axes, heads),
        grid=(near + 1,),
        in_specs=[
            pl.BlockSpec((1, positions, width), sequence),
            pl.BlockSpec((1, width), fixed(2)),
            pl.BlockSpec(w_key.shape, fixed(2)),
            pl.BlockSpec(w_value.shape, fixed(2)),
            pl.BlockSpec(queries.shape, fixed(3)),
            pl.BlockSpec(gates.shape, fixed(3)),
        ]
        + [pl.BlockSpec((positions, 2 * HD), fixed(2))] * heads,
        out_specs=[pl.BlockSpec((positions, 2 * HD), fixed(2))] * heads
        + [
            pl.BlockSpec((1, heads, positions, 2 * HD), lambda i: (jnp.maximum(i - 1, 0), 0, 0, 0)),
            pl.BlockSpec(tile_shape, fixed(3)),
            pl.BlockSpec(memory_space=pl.ANY),
        ],
        scratch_shapes=[pltpu.VMEM((heads, positions, 2 * HD), BF16)],
        out_shape=[jax.ShapeDtypeStruct((positions, 2 * HD), BF16)] * heads
        + [
            jax.ShapeDtypeStruct((near, heads, positions, 2 * HD), BF16),
            jax.ShapeDtypeStruct(tile_shape, F32),
            jax.ShapeDtypeStruct((seqs * heads * positions, 2 * HD), BF16),
        ],
        name="rest",
    )(tokens, norm_gain, w_key, w_value, queries, gates, *first)
    return made[:heads], *made[heads:]


def merge(tiles):
    both, best = merged(tiles)
    return packed(both, best, both[..., 1:2])


def after(value, *others):
    return lax.optimization_barrier((value,) + others)[0]


def read_beside(tokens, norm_gain, w_key, w_value, new_query, cum_gate):
    seqs, positions, _ = tokens.shape
    heads = w_key.shape[1] // HD
    query_heads = new_query.shape[1]
    group = query_heads // heads
    devices = seqs * heads
    half = seqs // 2
    everyone = ("hi", "lo", "tp")
    plane = lax.axis_index("hi") * half + lax.axis_index("lo")
    column = lax.axis_index("tp")
    near_first = lax.axis_index("hi") * half
    weights = (norm_gain, w_key, w_value)

    def swap(value, k, j):
        pairs = [(i, i ^ (k * heads + j)) for i in range(devices)]
        return lax.ppermute(value, everyone, pairs)

    first = make_across(everyone, half, tokens, *weights)
    arrived_first = [swap(first[0], half, 0)]
    gates = after(cum_gate.reshape(devices, positions // LANES, LANES), first[0])
    gates = lax.all_to_all(gates, everyone, split_axis=0, concat_axis=0, tiled=True)
    arrived_first += [swap(first[j], half, j) for j in range(1, heads)]
    queries = new_query.reshape(devices, group, HD)
    rest = make_rest(everyone, tokens, *weights, queries, gates, first)
    second, near, tile, cache = rest
    arrived_second = [swap(second[j], half + 1, j) for j in range(heads)]
    near = near.reshape(half * heads, positions, 2 * HD)
    arrived_near = lax.all_to_all(near, ("lo", "tp"), split_axis=0, concat_axis=0, tiled=True)
    rows = devices * positions

    def placed(cache, blocks, k, columns):
        for j in columns:
            start = ((plane ^ k) * heads + (column ^ j)) * positions
            cache = lax.dynamic_update_slice(cache, blocks[j], (start, 0))
        return cache

    columns = [1 << bit for bit in reversed(range(heads.bit_length() - 1))]
    for step, j in enumerate(columns):
        other = swap(tile, 0, j)
        if step == len(columns) - 1:
            cache = placed(cache, arrived_first, half, range(heads))
            other, cache = lax.optimization_barrier((other, cache))
        tile = merge([tile, other])
    others = [swap(tile, k, 0) for k in range(1, seqs)]
    near_rows = arrived_near.reshape(half * heads * positions, 2 * HD)
    cache = lax.dynamic_update_slice(cache, near_rows, (near_first * heads * positions, 0))
    cache = placed(cache, arrived_second, half + 1, range(heads - 1))
    others, cache = lax.optimization_barrier((others, cache))
    tile = merge([tile] + others)
    first_read = tile[..., HD:] / tile[..., 1:2]
    cache = placed(cache, arrived_second, half + 1, range(heads - 1, heads))
    return cache.reshape(1, 1, rows, 2 * HD), first_read.reshape(seqs, query_heads, HD)


def power_of_two(size):
    return size > 1 and size & (size - 1) == 0


def solution(mesh):
    groups, sp_count, tp_count = (mesh.shape[axis] for axis in ("gr", "sp", "tp"))
    sp_axes = "sp"
    halves_mesh = mesh
    if sp_count % 2 == 0:
        halves_mesh = jax.sharding.Mesh(
            mesh.devices.reshape(groups, 2, sp_count // 2, tp_count), ("gr", "hi", "lo", "tp")
        )
        sp_axes = ("hi", "lo")

    def shards(tokens, norm_gain, w_key, w_value, new_query, cum_gate):
        seqs, positions, width = tokens.shape
        heads = w_key.shape[1] // HD
        alone = sp_count == seqs and tp_count == heads
        even = power_of_two(seqs) and power_of_two(heads) and positions % LANES == 0
        body = read_beside if alone and even else functools.partial(read_after, sp_axes)
        return body(tokens, norm_gain.reshape(1, width), w_key, w_value, new_query, cum_gate)

    sp = sp_axes if isinstance(sp_axes, tuple) else (sp_axes,)
    in_specs = (
        P("gr", sp + ("tp",), None),
        P(),
        P(),
        P(),
        P("gr", None, None),
        P(("gr",) + sp, "tp", None),
    )
    out_specs = (P(("gr",) + sp, "tp", None, None), P("gr", None, None))
    return jax.shard_map(
        shards, mesh=halves_mesh, in_specs=in_specs, out_specs=out_specs, check_vma=False
    )
```

```python
import functools

import jax
import jax.numpy as jnp
from jax import lax
from jax.experimental import pallas as pl
from jax.experimental.pallas import tpu as pltpu
from jax.sharding import PartitionSpec as P

HD = 64
LANES = 128
NORM_FLOOR = 0.05
F32 = jnp.float32
BF16 = jnp.bfloat16


def divisor_up_to(total, limit):
    size = min(total, limit)
    while total % size:
        size -= 1
    return size


def normalize(tokens, gain):
    widened = tokens.astype(F32)
    mean_square = jnp.mean(widened * widened, axis=-1, keepdims=True)
    return (widened * lax.rsqrt(mean_square + NORM_FLOOR) * gain).astype(BF16)


def keys_and_values(normed, key_ref, value_ref):
    keys = jnp.dot(normed, key_ref[...], preferred_element_type=F32)
    values = jnp.dot(normed, value_ref[...], preferred_element_type=F32)
    for head in range(key_ref.shape[1] // HD):
        columns = slice(head * HD, (head + 1) * HD)
        yield head, jnp.concatenate([keys[:, columns], values[:, columns]], axis=-1).astype(BF16)


def three_parts(value, axis=0):
    high = value.astype(BF16)
    rest = value - high.astype(F32)
    middle = rest.astype(BF16)
    low = (rest - middle.astype(F32)).astype(BF16)
    return jnp.concatenate([high, middle, low], axis=axis)


def project_kernel(tokens_ref, gain_ref, key_ref, value_ref, out_ref):
    normed = normalize(tokens_ref[0], gain_ref[...])
    for head, both in keys_and_values(normed, key_ref, value_ref):
        out_ref[0, head] = both


def project(tokens, norm_gain, w_key, w_value):
    seqs, positions, width = tokens.shape
    heads = w_key.shape[1] // HD
    tile = divisor_up_to(positions, 512)
    return pl.pallas_call(
        project_kernel,
        grid=(seqs, positions // tile),
        in_specs=[
            pl.BlockSpec((1, tile, width), lambda s, i: (s, i, 0)),
            pl.BlockSpec((1, width), lambda s, i: (0, 0)),
            pl.BlockSpec(w_key.shape, lambda s, i: (0, 0)),
            pl.BlockSpec(w_value.shape, lambda s, i: (0, 0)),
        ],
        out_specs=pl.BlockSpec((1, heads, tile, 2 * HD), lambda s, i: (s, 0, i, 0)),
        out_shape=jax.ShapeDtypeStruct((seqs, heads, positions, 2 * HD), BF16),
        name="project",
    )(tokens, norm_gain, w_key, w_value)


def softmax_part(query, block, gate):
    rows = query.shape[0]
    scores = lax.dot_general(query, block, (((1,), (1,)), ((), ())), preferred_element_type=F32)
    scores = scores * HD ** (-0.5) - gate
    top = jnp.max(scores, axis=1, keepdims=True)
    weights = jnp.exp(scores - top)
    parts = jnp.dot(three_parts(weights), block, preferred_element_type=F32)
    summed = parts[:rows] + parts[rows : 2 * rows] + parts[2 * rows :]
    return summed, top, jnp.sum(weights, axis=1, keepdims=True)


def packed(summed, top, total):
    lane = lax.broadcasted_iota(jnp.int32, summed.shape, summed.ndim - 1)
    return jnp.where(lane >= HD, summed, jnp.where(lane == 0, top, total))


def merged(tiles):
    best = functools.reduce(jnp.maximum, [tile[..., :1] for tile in tiles])
    factors = [jnp.exp(tile[..., :1] - best) for tile in tiles]
    both = sum(tile * factor for tile, factor in zip(tiles, factors))
    return both, best


def read_kernel(chunks, query_ref, cache_ref, gate_ref, out_ref):
    size = cache_ref.shape[0] // chunks
    tiles = []
    for c in range(chunks):
        rows = slice(c * size, (c + 1) * size)
        tiles.append(packed(*softmax_part(query_ref[...], cache_ref[rows, :], gate_ref[:, rows])))
    both, best = merged(tiles)
    out_ref[...] = packed(both, best, both[:, 1:2])


def read(queries, cache, gates):
    padded = jnp.concatenate([queries, jnp.zeros_like(queries)], axis=-1)
    chunks = 4
    while cache.shape[0] % chunks:
        chunks -= 1
    return pl.pallas_call(
        functools.partial(read_kernel, chunks),
        out_shape=jax.ShapeDtypeStruct((queries.shape[0], 2 * HD), F32),
        name="read",
    )(padded, cache, gates)


def read_after(sp_axes, tokens, norm_gain, w_key, w_value, new_query, cum_gate):
    seqs, positions, _ = tokens.shape
    sp_count, tp_count = lax.axis_size(sp_axes), lax.axis_size("tp")
    everyone = (sp_axes if isinstance(sp_axes, tuple) else (sp_axes,)) + ("tp",)
    heads = w_key.shape[1] // HD
    classes, halves = sp_count // seqs, tp_count // heads
    piece = positions // (classes * halves)
    devices = sp_count * tp_count
    made = project(tokens, norm_gain, w_key, w_value)
    made = made.reshape(seqs, heads, classes, halves, piece, 2 * HD).transpose(0, 2, 1, 3, 4, 5)
    arrived = lax.all_to_all(
        made.reshape(devices, piece, 2 * HD), everyone, split_axis=0, concat_axis=0, tiled=True
    )
    kv_cache = arrived.reshape(devices * piece, 2 * HD)
    query_heads = new_query.shape[1]
    group = query_heads // heads
    seq_index = lax.axis_index(sp_axes) // classes
    head_index = lax.axis_index("tp") // halves
    queries = lax.dynamic_slice(new_query, (seq_index, head_index * group, 0), (1, group, HD))[0]
    tile = read(queries, kv_cache, cum_gate[0])
    tiles = lax.all_gather(tile, everyone)
    tiles = tiles.reshape(seqs, classes, heads, halves, group, 2 * HD)
    tops = tiles[..., :1]
    factors = jnp.exp(tops - jnp.max(tops, axis=(1, 3), keepdims=True))
    both = jnp.sum(tiles * factors, axis=(1, 3))
    first_read = both[..., HD:] / both[..., 1:2]
    return kv_cache[None, None], first_read.reshape(seqs, query_heads, HD)


def heads_made(normed, key_ref, value_ref):
    return [both for _, both in keys_and_values(normed, key_ref, value_ref)]


def across_kernel(axes, flip, tokens_ref, gain_ref, key_hbm, value_hbm, *refs):
    heads = len(refs) - 6
    out_refs, (token_ref, key_ref, value_ref, made_ref, loads, stores) = refs[:heads], refs[heads:]
    upper, lower, column = (lax.axis_index(axis) for axis in axes)
    seq = (upper * lax.axis_size(axes[1]) + lower) ^ flip
    pieces, rows = token_ref.shape[:2]
    moves = [(tokens_ref.at[seq, pl.ds(i * rows, rows)], token_ref.at[i]) for i in range(pieces)]
    moves += [(key_hbm, key_ref), (value_hbm, value_ref)]
    copies = [
        pltpu.make_async_copy(source, target, loads.at[i]) for i, (source, target) in enumerate(moves)
    ]
    for copy in copies:
        copy.start()
    normed = []
    for i in range(pieces):
        copies[i].wait()
        normed.append(normalize(token_ref[i], gain_ref[...]))
    copies[pieces].wait()
    keys = [jnp.dot(value, key_ref[...], preferred_element_type=F32) for value in normed]
    copies[pieces + 1].wait()
    writes = []
    for i in range(pieces):
        values = jnp.dot(normed[i], value_ref[...], preferred_element_type=F32)
        part = slice(i * rows, (i + 1) * rows)
        for head in range(heads):
            lanes = slice(head * HD, (head + 1) * HD)
            both = jnp.concatenate([keys[i][:, lanes], values[:, lanes]], axis=-1)
            made_ref[head, part] = both.astype(BF16)
        for j, out_ref in enumerate(out_refs):
            source = made_ref.at[column ^ j, pl.ds(i * rows, rows)]
            target = out_ref.at[pl.ds(i * rows, rows)]
            writes.append(pltpu.make_async_copy(source, target, stores.at[i, j]))
            writes[-1].start()
    for write in writes:
        write.wait()


def make_across(axes, flip, tokens, norm_gain, w_key, w_value):
    _, positions, width = tokens.shape
    heads = w_key.shape[1] // HD
    pieces = 2
    anywhere, vmem = pl.BlockSpec(memory_space=pl.ANY), pl.BlockSpec(memory_space=pltpu.VMEM)
    return pl.pallas_call(
        functools.partial(across_kernel, axes, flip),
        in_specs=[anywhere, vmem, anywhere, anywhere],
        out_specs=[anywhere] * heads,
        out_shape=[jax.ShapeDtypeStruct((positions, 2 * HD), BF16)] * heads,
        scratch_shapes=[
            pltpu.VMEM((pieces, positions // pieces, width), BF16),
            pltpu.VMEM(w_key.shape, BF16),
            pltpu.VMEM(w_value.shape, BF16),
            pltpu.VMEM((heads, positions, 2 * HD), BF16),
            pltpu.SemaphoreType.DMA((pieces + 2,)),
            pltpu.SemaphoreType.DMA((pieces, heads)),
        ],
        name="across",
    )(tokens, norm_gain, w_key, w_value)


def planes(axes):
    upper, lower, column = (lax.axis_index(axis) for axis in axes)
    half = lax.axis_size(axes[1])
    return upper * half + lower, upper * half, column, half


def read_sequence(slots, blocks, query_ref, gate_ref, tile_ref):
    heads, group = len(blocks), query_ref.shape[1]
    lanes, queries, gates = 2 * HD, [], []
    for head, slot in enumerate(slots):
        query = query_ref[slot].astype(F32)
        pieces = [jnp.zeros((group, size), F32) for size in (head * lanes, (heads - head) * lanes - HD)]
        pieces.insert(1, query)
        queries.append(jnp.concatenate([piece for piece in pieces if piece.shape[1]], axis=1))
        lines = gate_ref[slot]
        gate = jnp.concatenate([lines[i : i + 1] for i in range(lines.shape[0])], axis=1)
        gates.append(jnp.broadcast_to(gate, (group, gate.shape[1])))
    query = jnp.concatenate(queries, axis=0).astype(BF16)
    block = jnp.concatenate(blocks, axis=1)
    summed, top, total = softmax_part(query, block, jnp.concatenate(gates, axis=0))
    for head, slot in enumerate(slots):
        rows = slice(head * group, (head + 1) * group)
        columns = slice(head * lanes, (head + 1) * lanes)
        tile_ref[slot] = packed(summed[rows, columns], top[rows], total[rows])


def rest_kernel(axes, heads, tokens_ref, gain_ref, key_ref, value_ref, query_ref, gate_ref, *refs):
    first_refs, refs = refs[:heads], refs[heads:]
    second_refs, (near_ref, tile_ref, _, made_ref) = refs[:heads], refs[heads:]
    step = pl.program_id(0)
    plane, near_first, column, half = planes(axes)
    made = heads_made(normalize(tokens_ref[0], gain_ref[...]), key_ref, value_ref)
    seq = jnp.where(step == 0, plane ^ (half + 1), near_first + step - 1)
    slots = [seq * heads + head for head in range(heads)]
    read_sequence(slots, made, query_ref, gate_ref, tile_ref)

    @pl.when(step == 0)
    def _():
        for head, both in enumerate(made):
            made_ref[head] = both
        for j in range(heads):
            second_refs[j][...] = made_ref[column ^ j]
        slots = [(plane ^ half) * heads + (column ^ j) for j in range(heads)]
        read_sequence(slots, [ref[...] for ref in first_refs], query_ref, gate_ref, tile_ref)

    @pl.when(step > 0)
    def _():
        for head, both in enumerate(made):
            near_ref[0, head] = both


def make_rest(axes, tokens, norm_gain, w_key, w_value, queries, gates, first):
    seqs, positions, width = tokens.shape
    heads = w_key.shape[1] // HD
    near = seqs // 2
    fixed = lambda rank: lambda i: (0,) * rank
    tile_shape = queries.shape[:2] + (2 * HD,)

    def sequence(i):
        plane, near_first, _, half = planes(axes)
        return jnp.where(i == 0, plane ^ (half + 1), near_first + i - 1), 0, 0

    made = pl.pallas_call(
        functools.partial(rest_kernel, axes, heads),
        grid=(near + 1,),
        in_specs=[
            pl.BlockSpec((1, positions, width), sequence),
            pl.BlockSpec((1, width), fixed(2)),
            pl.BlockSpec(w_key.shape, fixed(2)),
            pl.BlockSpec(w_value.shape, fixed(2)),
            pl.BlockSpec(queries.shape, fixed(3)),
            pl.BlockSpec(gates.shape, fixed(3)),
        ]
        + [pl.BlockSpec((positions, 2 * HD), fixed(2))] * heads,
        out_specs=[pl.BlockSpec((positions, 2 * HD), fixed(2))] * heads
        + [
            pl.BlockSpec((1, heads, positions, 2 * HD), lambda i: (jnp.maximum(i - 1, 0), 0, 0, 0)),
            pl.BlockSpec(tile_shape, fixed(3)),
            pl.BlockSpec(memory_space=pl.ANY),
        ],
        scratch_shapes=[pltpu.VMEM((heads, positions, 2 * HD), BF16)],
        out_shape=[jax.ShapeDtypeStruct((positions, 2 * HD), BF16)] * heads
        + [
            jax.ShapeDtypeStruct((near, heads, positions, 2 * HD), BF16),
            jax.ShapeDtypeStruct(tile_shape, F32),
            jax.ShapeDtypeStruct((seqs * heads * positions, 2 * HD), BF16),
        ],
        name="rest",
    )(tokens, norm_gain, w_key, w_value, queries, gates, *first)
    return made[:heads], *made[heads:]


def merge(tiles):
    both, best = merged(tiles)
    return packed(both, best, both[..., 1:2])


def after(value, *others):
    return lax.optimization_barrier((value,) + others)[0]


def read_beside(tokens, norm_gain, w_key, w_value, new_query, cum_gate):
    seqs, positions, _ = tokens.shape
    heads = w_key.shape[1] // HD
    query_heads = new_query.shape[1]
    group = query_heads // heads
    devices = seqs * heads
    half = seqs // 2
    everyone = ("hi", "lo", "tp")
    plane = lax.axis_index("hi") * half + lax.axis_index("lo")
    column = lax.axis_index("tp")
    near_first = lax.axis_index("hi") * half
    weights = (norm_gain, w_key, w_value)

    def swap(value, k, j):
        pairs = [(i, i ^ (k * heads + j)) for i in range(devices)]
        return lax.ppermute(value, everyone, pairs)

    first = make_across(everyone, half, tokens, *weights)
    arrived_first = [swap(first[0], half, 0)]
    gates = after(cum_gate.reshape(devices, positions // LANES, LANES), first[0])
    gates = lax.all_to_all(gates, everyone, split_axis=0, concat_axis=0, tiled=True)
    arrived_first += [swap(first[j], half, j) for j in range(1, heads - 1)]
    last, gates = lax.optimization_barrier((first[-1], gates))
    arrived_first.append(swap(last, half, heads - 1))
    queries = new_query.reshape(devices, group, HD)
    rest = make_rest(everyone, tokens, *weights, queries, gates, first)
    second, near, tile, cache = rest
    arrived_second = [swap(second[j], half + 1, j) for j in range(heads)]
    near = near.reshape(half * heads, positions, 2 * HD)
    arrived_near = lax.all_to_all(near, ("lo", "tp"), split_axis=0, concat_axis=0, tiled=True)
    rows = devices * positions

    def placed(cache, blocks, k, columns):
        for j in columns:
            start = ((plane ^ k) * heads + (column ^ j)) * positions
            cache = lax.dynamic_update_slice(cache, blocks[j], (start, 0))
        return cache

    columns = [1 << bit for bit in reversed(range(1, heads.bit_length() - 1))]
    for j in columns:
        tile = merge([tile, swap(tile, 0, j)])
    odd = (column & 1) == 1
    low, high = tile[: devices // 2], tile[devices // 2 :]
    tile = jnp.where(odd, high, low)
    tile = merge([tile, swap(jnp.where(odd, low, high), 0, 1)])
    others = [swap(tile, k, 0) for k in range(1, seqs)]
    early = max(heads - 2, 0)
    cache = placed(cache, arrived_first, half, range(heads))
    cache = placed(cache, arrived_second, half + 1, range(early))
    near_rows = arrived_near.reshape(half * heads * positions, 2 * HD)
    cache = lax.dynamic_update_slice(cache, near_rows, (near_first * heads * positions, 0))
    cache = placed(cache, arrived_second, half + 1, range(early, heads - 1))
    others, cache = lax.optimization_barrier((others, cache))
    tile = merge([tile] + others)
    tile = tile / tile[..., 1:2]
    other = swap(tile, 0, 1)
    first_read = jnp.concatenate([jnp.where(odd, other, tile), jnp.where(odd, tile, other)])[..., HD:]
    cache = placed(cache, arrived_second, half + 1, range(heads - 1, heads))
    return cache.reshape(1, 1, rows, 2 * HD), first_read.reshape(seqs, query_heads, HD)


def power_of_two(size):
    return size > 1 and size & (size - 1) == 0


def solution(mesh):
    groups, sp_count, tp_count = (mesh.shape[axis] for axis in ("gr", "sp", "tp"))
    sp_axes = "sp"
    halves_mesh = mesh
    if sp_count % 2 == 0:
        halves_mesh = jax.sharding.Mesh(
            mesh.devices.reshape(groups, 2, sp_count // 2, tp_count), ("gr", "hi", "lo", "tp")
        )
        sp_axes = ("hi", "lo")

    def shards(tokens, norm_gain, w_key, w_value, new_query, cum_gate):
        seqs, positions, width = tokens.shape
        heads = w_key.shape[1] // HD
        alone = sp_count == seqs and tp_count == heads
        even = power_of_two(seqs) and power_of_two(heads) and positions % LANES == 0
        body = read_beside if alone and even else functools.partial(read_after, sp_axes)
        return body(tokens, norm_gain.reshape(1, width), w_key, w_value, new_query, cum_gate)

    sp = sp_axes if isinstance(sp_axes, tuple) else (sp_axes,)
    in_specs = (
        P("gr", sp + ("tp",), None),
        P(),
        P(),
        P(),
        P("gr", None, None),
        P(("gr",) + sp, "tp", None),
    )
    out_specs = (P(("gr",) + sp, "tp", None, None), P("gr", None, None))
    return jax.shard_map(
        shards, mesh=halves_mesh, in_specs=in_specs, out_specs=out_specs, check_vma=False
    )
```

```python
import functools

import jax
import jax.numpy as jnp
from jax import lax
from jax.experimental import pallas as pl
from jax.experimental.pallas import tpu as pltpu
from jax.sharding import PartitionSpec as P

HD = 64
LANES = 128
NORM_FLOOR = 0.05
F32 = jnp.float32
BF16 = jnp.bfloat16


def divisor_up_to(total, limit):
    size = min(total, limit)
    while total % size:
        size -= 1
    return size


def normalize(tokens, gain):
    widened = tokens.astype(F32)
    mean_square = jnp.mean(widened * widened, axis=-1, keepdims=True)
    return (widened * lax.rsqrt(mean_square + NORM_FLOOR) * gain).astype(BF16)


def keys_and_values(normed, key_ref, value_ref):
    keys = jnp.dot(normed, key_ref[...], preferred_element_type=F32)
    values = jnp.dot(normed, value_ref[...], preferred_element_type=F32)
    for head in range(key_ref.shape[1] // HD):
        columns = slice(head * HD, (head + 1) * HD)
        yield head, jnp.concatenate([keys[:, columns], values[:, columns]], axis=-1).astype(BF16)


def three_parts(value, axis=0):
    high = value.astype(BF16)
    rest = value - high.astype(F32)
    middle = rest.astype(BF16)
    low = (rest - middle.astype(F32)).astype(BF16)
    return jnp.concatenate([high, middle, low], axis=axis)


def project_kernel(tokens_ref, gain_ref, key_ref, value_ref, out_ref):
    normed = normalize(tokens_ref[0], gain_ref[...])
    for head, both in keys_and_values(normed, key_ref, value_ref):
        out_ref[0, head] = both


def project(tokens, norm_gain, w_key, w_value):
    seqs, positions, width = tokens.shape
    heads = w_key.shape[1] // HD
    tile = divisor_up_to(positions, 512)
    return pl.pallas_call(
        project_kernel,
        grid=(seqs, positions // tile),
        in_specs=[
            pl.BlockSpec((1, tile, width), lambda s, i: (s, i, 0)),
            pl.BlockSpec((1, width), lambda s, i: (0, 0)),
            pl.BlockSpec(w_key.shape, lambda s, i: (0, 0)),
            pl.BlockSpec(w_value.shape, lambda s, i: (0, 0)),
        ],
        out_specs=pl.BlockSpec((1, heads, tile, 2 * HD), lambda s, i: (s, 0, i, 0)),
        out_shape=jax.ShapeDtypeStruct((seqs, heads, positions, 2 * HD), BF16),
        name="project",
    )(tokens, norm_gain, w_key, w_value)


def softmax_part(query, block, gate):
    rows = query.shape[0]
    scores = lax.dot_general(query, block, (((1,), (1,)), ((), ())), preferred_element_type=F32)
    scores = scores * HD ** (-0.5) - gate
    top = jnp.max(scores, axis=1, keepdims=True)
    weights = jnp.exp(scores - top)
    parts = jnp.dot(three_parts(weights), block, preferred_element_type=F32)
    summed = parts[:rows] + parts[rows : 2 * rows] + parts[2 * rows :]
    return summed, top, jnp.sum(weights, axis=1, keepdims=True)


def packed(summed, top, total):
    lane = lax.broadcasted_iota(jnp.int32, summed.shape, summed.ndim - 1)
    return jnp.where(lane >= HD, summed, jnp.where(lane == 0, top, total))


def merged(tiles):
    best = functools.reduce(jnp.maximum, [tile[..., :1] for tile in tiles])
    factors = [jnp.exp(tile[..., :1] - best) for tile in tiles]
    both = sum(tile * factor for tile, factor in zip(tiles, factors))
    return both, best


def read_kernel(chunks, query_ref, cache_ref, gate_ref, out_ref):
    size = cache_ref.shape[0] // chunks
    tiles = []
    for c in range(chunks):
        rows = slice(c * size, (c + 1) * size)
        tiles.append(packed(*softmax_part(query_ref[...], cache_ref[rows, :], gate_ref[:, rows])))
    both, best = merged(tiles)
    out_ref[...] = packed(both, best, both[:, 1:2])


def read(queries, cache, gates):
    padded = jnp.concatenate([queries, jnp.zeros_like(queries)], axis=-1)
    chunks = 4
    while cache.shape[0] % chunks:
        chunks -= 1
    return pl.pallas_call(
        functools.partial(read_kernel, chunks),
        out_shape=jax.ShapeDtypeStruct((queries.shape[0], 2 * HD), F32),
        name="read",
    )(padded, cache, gates)


def read_after(sp_axes, tokens, norm_gain, w_key, w_value, new_query, cum_gate):
    seqs, positions, _ = tokens.shape
    sp_count, tp_count = lax.axis_size(sp_axes), lax.axis_size("tp")
    everyone = (sp_axes if isinstance(sp_axes, tuple) else (sp_axes,)) + ("tp",)
    heads = w_key.shape[1] // HD
    classes, halves = sp_count // seqs, tp_count // heads
    piece = positions // (classes * halves)
    devices = sp_count * tp_count
    made = project(tokens, norm_gain, w_key, w_value)
    made = made.reshape(seqs, heads, classes, halves, piece, 2 * HD).transpose(0, 2, 1, 3, 4, 5)
    arrived = lax.all_to_all(
        made.reshape(devices, piece, 2 * HD), everyone, split_axis=0, concat_axis=0, tiled=True
    )
    kv_cache = arrived.reshape(devices * piece, 2 * HD)
    query_heads = new_query.shape[1]
    group = query_heads // heads
    seq_index = lax.axis_index(sp_axes) // classes
    head_index = lax.axis_index("tp") // halves
    queries = lax.dynamic_slice(new_query, (seq_index, head_index * group, 0), (1, group, HD))[0]
    tile = read(queries, kv_cache, cum_gate[0])
    tiles = lax.all_gather(tile, everyone)
    tiles = tiles.reshape(seqs, classes, heads, halves, group, 2 * HD)
    tops = tiles[..., :1]
    factors = jnp.exp(tops - jnp.max(tops, axis=(1, 3), keepdims=True))
    both = jnp.sum(tiles * factors, axis=(1, 3))
    first_read = both[..., HD:] / both[..., 1:2]
    return kv_cache[None, None], first_read.reshape(seqs, query_heads, HD)


def heads_made(normed, key_ref, value_ref):
    return [both for _, both in keys_and_values(normed, key_ref, value_ref)]


def across_kernel(axes, flip, tokens_ref, gain_ref, key_hbm, value_hbm, *refs):
    heads = len(refs) - 5
    out_refs, (token_ref, weight_ref, made_ref, loads, stores) = refs[:heads], refs[heads:]
    upper, lower, column = (lax.axis_index(axis) for axis in axes)
    seq = (upper * lax.axis_size(axes[1]) + lower) ^ flip
    pieces, rows = token_ref.shape[:2]
    moves = [(tokens_ref.at[seq, pl.ds(i * rows, rows)], token_ref.at[i]) for i in range(pieces)]
    wide = key_hbm.shape[1]
    moves += [(key_hbm, weight_ref.at[:, pl.ds(0, wide)]), (value_hbm, weight_ref.at[:, pl.ds(wide, wide)])]
    copies = [
        pltpu.make_async_copy(source, target, loads.at[i]) for i, (source, target) in enumerate(moves)
    ]
    for copy in copies:
        copy.start()
    normed = []
    for i in range(pieces):
        copies[i].wait()
        normed.append(normalize(token_ref[i], gain_ref[...]))
    copies[pieces].wait()
    copies[pieces + 1].wait()
    writes = []
    for i in range(pieces):
        made = jnp.dot(normed[i], weight_ref[...], preferred_element_type=F32)
        part = slice(i * rows, (i + 1) * rows)
        for head in range(heads):
            k = made[:, head * HD : (head + 1) * HD]
            v = made[:, wide + head * HD : wide + (head + 1) * HD]
            made_ref[head, part] = jnp.concatenate([k, v], axis=-1).astype(BF16)
        for j, out_ref in enumerate(out_refs):
            source = made_ref.at[column ^ j, pl.ds(i * rows, rows)]
            target = out_ref.at[pl.ds(i * rows, rows)]
            writes.append(pltpu.make_async_copy(source, target, stores.at[i, j]))
            writes[-1].start()
    for write in writes:
        write.wait()


def make_across(axes, flip, tokens, norm_gain, w_key, w_value):
    _, positions, width = tokens.shape
    heads = w_key.shape[1] // HD
    pieces = 2
    anywhere, vmem = pl.BlockSpec(memory_space=pl.ANY), pl.BlockSpec(memory_space=pltpu.VMEM)
    return pl.pallas_call(
        functools.partial(across_kernel, axes, flip),
        in_specs=[anywhere, vmem, anywhere, anywhere],
        out_specs=[anywhere] * heads,
        out_shape=[jax.ShapeDtypeStruct((positions, 2 * HD), BF16)] * heads,
        scratch_shapes=[
            pltpu.VMEM((pieces, positions // pieces, width), BF16),
            pltpu.VMEM((width, 2 * w_key.shape[1]), BF16),
            pltpu.VMEM((heads, positions, 2 * HD), BF16),
            pltpu.SemaphoreType.DMA((pieces + 2,)),
            pltpu.SemaphoreType.DMA((pieces, heads)),
        ],
        name="across",
    )(tokens, norm_gain, w_key, w_value)


def planes(axes):
    upper, lower, column = (lax.axis_index(axis) for axis in axes)
    half = lax.axis_size(axes[1])
    return upper * half + lower, upper * half, column, half


def read_sequence(slots, blocks, query_ref, gate_ref, tile_ref):
    heads, group = len(blocks), query_ref.shape[1]
    lanes, queries, gates = 2 * HD, [], []
    for head, slot in enumerate(slots):
        query = query_ref[slot].astype(F32)
        pieces = [jnp.zeros((group, size), F32) for size in (head * lanes, (heads - head) * lanes - HD)]
        pieces.insert(1, query)
        queries.append(jnp.concatenate([piece for piece in pieces if piece.shape[1]], axis=1))
        lines = gate_ref[slot]
        gate = jnp.concatenate([lines[i : i + 1] for i in range(lines.shape[0])], axis=1)
        gates.append(jnp.broadcast_to(gate, (group, gate.shape[1])))
    query = jnp.concatenate(queries, axis=0).astype(BF16)
    block = jnp.concatenate(blocks, axis=1)
    summed, top, total = softmax_part(query, block, jnp.concatenate(gates, axis=0))
    for head, slot in enumerate(slots):
        rows = slice(head * group, (head + 1) * group)
        columns = slice(head * lanes, (head + 1) * lanes)
        tile_ref[slot] = packed(summed[rows, columns], top[rows], total[rows])


def rest_kernel(axes, heads, tokens_ref, gain_ref, key_ref, value_ref, query_ref, gate_ref, *refs):
    first_refs, refs = refs[:heads], refs[heads:]
    second_refs, (near_ref, tile_ref, _, made_ref) = refs[:heads], refs[heads:]
    step = pl.program_id(0)
    plane, near_first, column, half = planes(axes)
    made = heads_made(normalize(tokens_ref[0], gain_ref[...]), key_ref, value_ref)
    seq = jnp.where(step == 0, plane ^ (half + 1), near_first + step - 1)
    slots = [seq * heads + head for head in range(heads)]
    read_sequence(slots, made, query_ref, gate_ref, tile_ref)

    @pl.when(step == 0)
    def _():
        for head, both in enumerate(made):
            made_ref[head] = both
        for j in range(heads):
            second_refs[j][...] = made_ref[column ^ j]
        slots = [(plane ^ half) * heads + (column ^ j) for j in range(heads)]
        read_sequence(slots, [ref[...] for ref in first_refs], query_ref, gate_ref, tile_ref)

    @pl.when(step > 0)
    def _():
        for head, both in enumerate(made):
            near_ref[0, head] = both


def make_rest(axes, tokens, norm_gain, w_key, w_value, queries, gates, first):
    seqs, positions, width = tokens.shape
    heads = w_key.shape[1] // HD
    near = seqs // 2
    fixed = lambda rank: lambda i: (0,) * rank
    tile_shape = queries.shape[:2] + (2 * HD,)

    def sequence(i):
        plane, near_first, _, half = planes(axes)
        return jnp.where(i == 0, plane ^ (half + 1), near_first + i - 1), 0, 0

    made = pl.pallas_call(
        functools.partial(rest_kernel, axes, heads),
        grid=(near + 1,),
        in_specs=[
            pl.BlockSpec((1, positions, width), sequence),
            pl.BlockSpec((1, width), fixed(2)),
            pl.BlockSpec(w_key.shape, fixed(2)),
            pl.BlockSpec(w_value.shape, fixed(2)),
            pl.BlockSpec(queries.shape, fixed(3)),
            pl.BlockSpec(gates.shape, fixed(3)),
        ]
        + [pl.BlockSpec((positions, 2 * HD), fixed(2))] * heads,
        out_specs=[pl.BlockSpec((positions, 2 * HD), fixed(2))] * heads
        + [
            pl.BlockSpec((1, heads, positions, 2 * HD), lambda i: (jnp.maximum(i - 1, 0), 0, 0, 0)),
            pl.BlockSpec(tile_shape, fixed(3)),
            pl.BlockSpec(memory_space=pl.ANY),
        ],
        scratch_shapes=[pltpu.VMEM((heads, positions, 2 * HD), BF16)],
        out_shape=[jax.ShapeDtypeStruct((positions, 2 * HD), BF16)] * heads
        + [
            jax.ShapeDtypeStruct((near, heads, positions, 2 * HD), BF16),
            jax.ShapeDtypeStruct(tile_shape, F32),
            jax.ShapeDtypeStruct((seqs * heads * positions, 2 * HD), BF16),
        ],
        name="rest",
    )(tokens, norm_gain, w_key, w_value, queries, gates, *first)
    return made[:heads], *made[heads:]


def merge(tiles):
    both, best = merged(tiles)
    return packed(both, best, both[..., 1:2])


def after(value, *others):
    return lax.optimization_barrier((value,) + others)[0]


def read_beside(tokens, norm_gain, w_key, w_value, new_query, cum_gate):
    seqs, positions, _ = tokens.shape
    heads = w_key.shape[1] // HD
    query_heads = new_query.shape[1]
    group = query_heads // heads
    devices = seqs * heads
    half = seqs // 2
    everyone = ("hi", "lo", "tp")
    plane = lax.axis_index("hi") * half + lax.axis_index("lo")
    column = lax.axis_index("tp")
    near_first = lax.axis_index("hi") * half
    weights = (norm_gain, w_key, w_value)

    def swap(value, k, j):
        pairs = [(i, i ^ (k * heads + j)) for i in range(devices)]
        return lax.ppermute(value, everyone, pairs)

    first = make_across(everyone, half, tokens, *weights)
    gates = after(cum_gate.reshape(devices, positions // LANES, LANES), first[0])
    gates = lax.all_to_all(gates, everyone, split_axis=0, concat_axis=0, tiled=True)
    ready, gates = lax.optimization_barrier((first[3], gates))
    blocks = [ready if j == 3 else block for j, block in enumerate(first)]
    arrived_first = [swap(block, half, j) for j, block in enumerate(blocks)]
    queries = new_query.reshape(devices, group, HD)
    rest = make_rest(everyone, tokens, *weights, queries, gates, first)
    second, near, tile, cache = rest
    arrived_second = [swap(second[j], half + 1, j) for j in range(heads)]
    near = near.reshape(half * heads, positions, 2 * HD)
    arrived_near = lax.all_to_all(near, ("lo", "tp"), split_axis=0, concat_axis=0, tiled=True)
    rows = devices * positions

    def placed(cache, blocks, k):
        for bit in range(heads.bit_length() - 1):
            swapped = ((column >> bit) & 1) == 1
            blocks = [
                jnp.where(swapped, blocks[head ^ (1 << bit)], block)
                for head, block in enumerate(blocks)
            ]
        start = (plane ^ k) * heads * positions
        return lax.dynamic_update_slice(cache, jnp.concatenate(blocks), (start, 0))

    columns = [1 << bit for bit in reversed(range(1, heads.bit_length() - 1))]
    for j in columns:
        tile = merge([tile, swap(tile, 0, j)])
    odd = (column & 1) == 1
    low, high = tile[: devices // 2], tile[devices // 2 :]
    tile = jnp.where(odd, high, low)
    tile = merge([tile, swap(jnp.where(odd, low, high), 0, 1)])
    others = [swap(tile, k, 0) for k in range(1, seqs)]
    cache = placed(cache, arrived_first, half)
    near_rows = arrived_near.reshape(half * heads * positions, 2 * HD)
    cache = lax.dynamic_update_slice(cache, near_rows, (near_first * heads * positions, 0))
    tile = merge([tile] + others)
    tile = tile / tile[..., 1:2]
    other = swap(tile, 0, 1)
    pair = [jnp.where(odd, other, tile), jnp.where(odd, tile, other)]
    first_read = jnp.concatenate(pair)[..., HD:]
    cache = placed(cache, arrived_second, half + 1)
    return cache.reshape(1, 1, rows, 2 * HD), first_read.reshape(seqs, query_heads, HD)


def power_of_two(size):
    return size > 1 and size & (size - 1) == 0


def solution(mesh):
    groups, sp_count, tp_count = (mesh.shape[axis] for axis in ("gr", "sp", "tp"))
    sp_axes = "sp"
    halves_mesh = mesh
    if sp_count % 2 == 0:
        halves_mesh = jax.sharding.Mesh(
            mesh.devices.reshape(groups, 2, sp_count // 2, tp_count), ("gr", "hi", "lo", "tp")
        )
        sp_axes = ("hi", "lo")

    def shards(tokens, norm_gain, w_key, w_value, new_query, cum_gate):
        seqs, positions, width = tokens.shape
        heads = w_key.shape[1] // HD
        alone = sp_count == seqs and tp_count == heads
        even = power_of_two(seqs) and power_of_two(heads) and positions % LANES == 0
        body = read_beside if alone and even and seqs // 2 == 2 else functools.partial(read_after, sp_axes)
        return body(tokens, norm_gain.reshape(1, width), w_key, w_value, new_query, cum_gate)

    sp = sp_axes if isinstance(sp_axes, tuple) else (sp_axes,)
    in_specs = (
        P("gr", sp + ("tp",), None),
        P(),
        P(),
        P(),
        P("gr", None, None),
        P(("gr",) + sp, "tp", None),
    )
    out_specs = (P(("gr",) + sp, "tp", None, None), P("gr", None, None))
    return jax.shard_map(
        shards, mesh=halves_mesh, in_specs=in_specs, out_specs=out_specs, check_vma=False
    )
```

```python
import functools

import jax
import jax.numpy as jnp
from jax import lax
from jax.experimental import pallas as pl
from jax.experimental.pallas import tpu as pltpu
from jax.sharding import PartitionSpec as P

HD = 64
LANES = 128
NORM_FLOOR = 0.05
F32 = jnp.float32
BF16 = jnp.bfloat16


def divisor_up_to(total, limit):
    size = min(total, limit)
    while total % size:
        size -= 1
    return size


def normalize(tokens, gain):
    widened = tokens.astype(F32)
    mean_square = jnp.mean(widened * widened, axis=-1, keepdims=True)
    return (widened * lax.rsqrt(mean_square + NORM_FLOOR) * gain).astype(BF16)


def keys_and_values(normed, key_ref, value_ref):
    keys = jnp.dot(normed, key_ref[...], preferred_element_type=F32)
    values = jnp.dot(normed, value_ref[...], preferred_element_type=F32)
    for head in range(key_ref.shape[1] // HD):
        columns = slice(head * HD, (head + 1) * HD)
        yield head, jnp.concatenate([keys[:, columns], values[:, columns]], axis=-1).astype(BF16)


def three_parts(value, axis=0):
    high = value.astype(BF16)
    rest = value - high.astype(F32)
    middle = rest.astype(BF16)
    low = (rest - middle.astype(F32)).astype(BF16)
    return jnp.concatenate([high, middle, low], axis=axis)


def project_kernel(tokens_ref, gain_ref, key_ref, value_ref, out_ref):
    normed = normalize(tokens_ref[0], gain_ref[...])
    for head, both in keys_and_values(normed, key_ref, value_ref):
        out_ref[0, head] = both


def project(tokens, norm_gain, w_key, w_value):
    seqs, positions, width = tokens.shape
    heads = w_key.shape[1] // HD
    tile = divisor_up_to(positions, 512)
    return pl.pallas_call(
        project_kernel,
        grid=(seqs, positions // tile),
        in_specs=[
            pl.BlockSpec((1, tile, width), lambda s, i: (s, i, 0)),
            pl.BlockSpec((1, width), lambda s, i: (0, 0)),
            pl.BlockSpec(w_key.shape, lambda s, i: (0, 0)),
            pl.BlockSpec(w_value.shape, lambda s, i: (0, 0)),
        ],
        out_specs=pl.BlockSpec((1, heads, tile, 2 * HD), lambda s, i: (s, 0, i, 0)),
        out_shape=jax.ShapeDtypeStruct((seqs, heads, positions, 2 * HD), BF16),
        name="project",
    )(tokens, norm_gain, w_key, w_value)


def softmax_part(query, block, gate):
    rows = query.shape[0]
    scores = lax.dot_general(query, block, (((1,), (1,)), ((), ())), preferred_element_type=F32)
    scores = scores * HD ** (-0.5) - gate
    top = jnp.max(scores, axis=1, keepdims=True)
    weights = jnp.exp(scores - top)
    parts = jnp.dot(three_parts(weights), block, preferred_element_type=F32)
    summed = parts[:rows] + parts[rows : 2 * rows] + parts[2 * rows :]
    return summed, top, jnp.sum(weights, axis=1, keepdims=True)


def packed(summed, top, total):
    lane = lax.broadcasted_iota(jnp.int32, summed.shape, summed.ndim - 1)
    return jnp.where(lane >= HD, summed, jnp.where(lane == 0, top, total))


def merged(tiles):
    best = functools.reduce(jnp.maximum, [tile[..., :1] for tile in tiles])
    factors = [jnp.exp(tile[..., :1] - best) for tile in tiles]
    both = sum(tile * factor for tile, factor in zip(tiles, factors))
    return both, best


def read_kernel(chunks, query_ref, cache_ref, gate_ref, out_ref):
    size = cache_ref.shape[0] // chunks
    tiles = []
    for c in range(chunks):
        rows = slice(c * size, (c + 1) * size)
        tiles.append(packed(*softmax_part(query_ref[...], cache_ref[rows, :], gate_ref[:, rows])))
    both, best = merged(tiles)
    out_ref[...] = packed(both, best, both[:, 1:2])


def read(queries, cache, gates):
    padded = jnp.concatenate([queries, jnp.zeros_like(queries)], axis=-1)
    chunks = 4
    while cache.shape[0] % chunks:
        chunks -= 1
    return pl.pallas_call(
        functools.partial(read_kernel, chunks),
        out_shape=jax.ShapeDtypeStruct((queries.shape[0], 2 * HD), F32),
        name="read",
    )(padded, cache, gates)


def read_after(sp_axes, tokens, norm_gain, w_key, w_value, new_query, cum_gate):
    seqs, positions, _ = tokens.shape
    sp_count, tp_count = lax.axis_size(sp_axes), lax.axis_size("tp")
    everyone = (sp_axes if isinstance(sp_axes, tuple) else (sp_axes,)) + ("tp",)
    heads = w_key.shape[1] // HD
    classes, halves = sp_count // seqs, tp_count // heads
    piece = positions // (classes * halves)
    devices = sp_count * tp_count
    made = project(tokens, norm_gain, w_key, w_value)
    made = made.reshape(seqs, heads, classes, halves, piece, 2 * HD).transpose(0, 2, 1, 3, 4, 5)
    arrived = lax.all_to_all(
        made.reshape(devices, piece, 2 * HD), everyone, split_axis=0, concat_axis=0, tiled=True
    )
    kv_cache = arrived.reshape(devices * piece, 2 * HD)
    query_heads = new_query.shape[1]
    group = query_heads // heads
    seq_index = lax.axis_index(sp_axes) // classes
    head_index = lax.axis_index("tp") // halves
    queries = lax.dynamic_slice(new_query, (seq_index, head_index * group, 0), (1, group, HD))[0]
    tile = read(queries, kv_cache, cum_gate[0])
    tiles = lax.all_gather(tile, everyone)
    tiles = tiles.reshape(seqs, classes, heads, halves, group, 2 * HD)
    tops = tiles[..., :1]
    factors = jnp.exp(tops - jnp.max(tops, axis=(1, 3), keepdims=True))
    both = jnp.sum(tiles * factors, axis=(1, 3))
    first_read = both[..., HD:] / both[..., 1:2]
    return kv_cache[None, None], first_read.reshape(seqs, query_heads, HD)


def heads_made(normed, key_ref, value_ref):
    return [both for _, both in keys_and_values(normed, key_ref, value_ref)]


def across_kernel(axes, flip, tokens_ref, gain_ref, key_hbm, value_hbm, *refs):
    heads = len(refs) - 5
    out_refs, (token_ref, weight_ref, made_ref, loads, stores) = refs[:heads], refs[heads:]
    upper, lower, column = (lax.axis_index(axis) for axis in axes)
    seq = (upper * lax.axis_size(axes[1]) + lower) ^ flip
    pieces, rows = token_ref.shape[:2]
    moves = [(tokens_ref.at[seq, pl.ds(i * rows, rows)], token_ref.at[i]) for i in range(pieces)]
    wide = key_hbm.shape[1]
    moves += [(key_hbm, weight_ref.at[:, pl.ds(0, wide)]), (value_hbm, weight_ref.at[:, pl.ds(wide, wide)])]
    copies = [
        pltpu.make_async_copy(source, target, loads.at[i]) for i, (source, target) in enumerate(moves)
    ]
    for copy in copies:
        copy.start()
    normed = []
    for i in range(pieces):
        copies[i].wait()
        normed.append(normalize(token_ref[i], gain_ref[...]))
    copies[pieces].wait()
    copies[pieces + 1].wait()
    writes = []
    for i in range(pieces):
        made = jnp.dot(normed[i], weight_ref[...], preferred_element_type=F32)
        part = slice(i * rows, (i + 1) * rows)
        for head in range(heads):
            k = made[:, head * HD : (head + 1) * HD]
            v = made[:, wide + head * HD : wide + (head + 1) * HD]
            made_ref[head, part] = jnp.concatenate([k, v], axis=-1).astype(BF16)
        for j, out_ref in enumerate(out_refs):
            source = made_ref.at[column ^ j, pl.ds(i * rows, rows)]
            target = out_ref.at[pl.ds(i * rows, rows)]
            writes.append(pltpu.make_async_copy(source, target, stores.at[i, j]))
            writes[-1].start()
    for write in writes:
        write.wait()


def make_across(axes, flip, tokens, norm_gain, w_key, w_value):
    _, positions, width = tokens.shape
    heads = w_key.shape[1] // HD
    pieces = 2
    anywhere, vmem = pl.BlockSpec(memory_space=pl.ANY), pl.BlockSpec(memory_space=pltpu.VMEM)
    return pl.pallas_call(
        functools.partial(across_kernel, axes, flip),
        in_specs=[anywhere, vmem, anywhere, anywhere],
        out_specs=[anywhere] * heads,
        out_shape=[jax.ShapeDtypeStruct((positions, 2 * HD), BF16)] * heads,
        scratch_shapes=[
            pltpu.VMEM((pieces, positions // pieces, width), BF16),
            pltpu.VMEM((width, 2 * w_key.shape[1]), BF16),
            pltpu.VMEM((heads, positions, 2 * HD), BF16),
            pltpu.SemaphoreType.DMA((pieces + 2,)),
            pltpu.SemaphoreType.DMA((pieces, heads)),
        ],
        name="across",
    )(tokens, norm_gain, w_key, w_value)


def planes(axes):
    upper, lower, column = (lax.axis_index(axis) for axis in axes)
    half = lax.axis_size(axes[1])
    return upper * half + lower, upper * half, column, half


def read_sequence(slots, blocks, query_ref, gate_ref, tile_ref):
    heads, group = len(blocks), query_ref.shape[1]
    lanes, queries, gates = 2 * HD, [], []
    for head, slot in enumerate(slots):
        query = query_ref[slot].astype(F32)
        pieces = [jnp.zeros((group, size), F32) for size in (head * lanes, (heads - head) * lanes - HD)]
        pieces.insert(1, query)
        queries.append(jnp.concatenate([piece for piece in pieces if piece.shape[1]], axis=1))
        lines = gate_ref[slot]
        gate = jnp.concatenate([lines[i : i + 1] for i in range(lines.shape[0])], axis=1)
        gates.append(jnp.broadcast_to(gate, (group, gate.shape[1])))
    query = jnp.concatenate(queries, axis=0).astype(BF16)
    block = jnp.concatenate(blocks, axis=1)
    summed, top, total = softmax_part(query, block, jnp.concatenate(gates, axis=0))
    for head, slot in enumerate(slots):
        rows = slice(head * group, (head + 1) * group)
        columns = slice(head * lanes, (head + 1) * lanes)
        tile_ref[slot] = packed(summed[rows, columns], top[rows], total[rows])


def rest_kernel(axes, heads, tokens_ref, gain_ref, key_ref, value_ref, query_ref, gate_ref, *refs):
    first_refs, refs = refs[:heads], refs[heads:]
    second_refs, (near_ref, tile_ref, _, made_ref) = refs[:heads], refs[heads:]
    step = pl.program_id(0)
    plane, near_first, column, half = planes(axes)
    made = heads_made(normalize(tokens_ref[0], gain_ref[...]), key_ref, value_ref)
    seq = jnp.where(step == 0, plane ^ (half + 1), near_first + step - 1)
    slots = [seq * heads + head for head in range(heads)]
    read_sequence(slots, made, query_ref, gate_ref, tile_ref)

    @pl.when(step == 0)
    def _():
        for head, both in enumerate(made):
            made_ref[head] = both
        for j in range(heads):
            second_refs[j][...] = made_ref[column ^ j]
        slots = [(plane ^ half) * heads + (column ^ j) for j in range(heads)]
        read_sequence(slots, [ref[...] for ref in first_refs], query_ref, gate_ref, tile_ref)

    @pl.when(step > 0)
    def _():
        for head, both in enumerate(made):
            near_ref[0, head] = both


def make_rest(axes, tokens, norm_gain, w_key, w_value, queries, gates, first):
    seqs, positions, width = tokens.shape
    heads = w_key.shape[1] // HD
    near = seqs // 2
    fixed = lambda rank: lambda i: (0,) * rank
    tile_shape = queries.shape[:2] + (2 * HD,)

    def sequence(i):
        plane, near_first, _, half = planes(axes)
        return jnp.where(i == 0, plane ^ (half + 1), near_first + i - 1), 0, 0

    made = pl.pallas_call(
        functools.partial(rest_kernel, axes, heads),
        grid=(near + 1,),
        in_specs=[
            pl.BlockSpec((1, positions, width), sequence),
            pl.BlockSpec((1, width), fixed(2)),
            pl.BlockSpec(w_key.shape, fixed(2)),
            pl.BlockSpec(w_value.shape, fixed(2)),
            pl.BlockSpec(queries.shape, fixed(3)),
            pl.BlockSpec(gates.shape, fixed(3)),
        ]
        + [pl.BlockSpec((positions, 2 * HD), fixed(2))] * heads,
        out_specs=[pl.BlockSpec((positions, 2 * HD), fixed(2))] * heads
        + [
            pl.BlockSpec((1, heads, positions, 2 * HD), lambda i: (jnp.maximum(i - 1, 0), 0, 0, 0)),
            pl.BlockSpec(tile_shape, fixed(3)),
            pl.BlockSpec(memory_space=pl.ANY),
        ],
        scratch_shapes=[pltpu.VMEM((heads, positions, 2 * HD), BF16)],
        out_shape=[jax.ShapeDtypeStruct((positions, 2 * HD), BF16)] * heads
        + [
            jax.ShapeDtypeStruct((near, heads, positions, 2 * HD), BF16),
            jax.ShapeDtypeStruct(tile_shape, F32),
            jax.ShapeDtypeStruct((seqs * heads * positions, 2 * HD), BF16),
        ],
        name="rest",
    )(tokens, norm_gain, w_key, w_value, queries, gates, *first)
    return made[:heads], *made[heads:]


def merge(tiles):
    both, best = merged(tiles)
    return packed(both, best, both[..., 1:2])


def after(value, *others):
    return lax.optimization_barrier((value,) + others)[0]


def read_beside(tokens, norm_gain, w_key, w_value, new_query, cum_gate):
    seqs, positions, _ = tokens.shape
    heads = w_key.shape[1] // HD
    query_heads = new_query.shape[1]
    group = query_heads // heads
    devices = seqs * heads
    half = seqs // 2
    everyone = ("hi", "lo", "tp")
    plane = lax.axis_index("hi") * half + lax.axis_index("lo")
    column = lax.axis_index("tp")
    near_first = lax.axis_index("hi") * half
    weights = (norm_gain, w_key, w_value)

    def swap(value, k, j):
        pairs = [(i, i ^ (k * heads + j)) for i in range(devices)]
        return lax.ppermute(value, everyone, pairs)

    first = make_across(everyone, half, tokens, *weights)
    gates = after(cum_gate.reshape(devices, positions // LANES, LANES), first[0])
    gates = lax.all_to_all(gates, everyone, split_axis=0, concat_axis=0, tiled=True)
    ready, gates = lax.optimization_barrier((first[3], gates))
    blocks = [ready if j == 3 else block for j, block in enumerate(first)]
    arrived_first = [swap(block, half, j) for j, block in enumerate(blocks)]
    queries = new_query.reshape(devices, group, HD)
    rest = make_rest(everyone, tokens, *weights, queries, gates, first)
    second, near, tile, cache = rest
    arrived_second = [swap(second[j], half + 1, j) for j in range(heads)]
    near = near.reshape(half * heads, positions, 2 * HD)
    arrived_near = lax.all_to_all(near, ("lo", "tp"), split_axis=0, concat_axis=0, tiled=True)
    rows = devices * positions

    def placed(cache, blocks, k):
        for bit in range(heads.bit_length() - 1):
            swapped = ((column >> bit) & 1) == 1
            blocks = [
                jnp.where(swapped, blocks[head ^ (1 << bit)], block)
                for head, block in enumerate(blocks)
            ]
        start = (plane ^ k) * heads * positions
        return lax.dynamic_update_slice(cache, jnp.concatenate(blocks), (start, 0))

    def placed_alone(cache, block, k, j):
        start = ((plane ^ k) * heads + (column ^ j)) * positions
        return lax.dynamic_update_slice(cache, block, (start, 0))

    columns = [1 << bit for bit in reversed(range(1, heads.bit_length() - 1))]
    for j in columns:
        tile = merge([tile, swap(tile, 0, j)])
    odd = (column & 1) == 1
    low, high = tile[: devices // 2], tile[devices // 2 :]
    tile = jnp.where(odd, high, low)
    tile = merge([tile, swap(jnp.where(odd, low, high), 0, 1)])
    others = [swap(tile, k, 0) for k in range(1, seqs)]
    cache = placed(cache, arrived_first, half)
    for j, block in enumerate(arrived_second[:-1]):
        cache = placed_alone(cache, block, half + 1, j)
    near_rows = arrived_near.reshape(half * heads * positions, 2 * HD)
    cache = lax.dynamic_update_slice(cache, near_rows, (near_first * heads * positions, 0))
    tile = merge([tile] + others)
    tile = tile / tile[..., 1:2]
    other = swap(tile, 0, 1)
    pair = [jnp.where(odd, other, tile), jnp.where(odd, tile, other)]
    first_read = jnp.concatenate(pair)[..., HD:]
    cache = placed_alone(cache, arrived_second[-1], half + 1, heads - 1)
    return cache.reshape(1, 1, rows, 2 * HD), first_read.reshape(seqs, query_heads, HD)


def power_of_two(size):
    return size > 1 and size & (size - 1) == 0


def solution(mesh):
    groups, sp_count, tp_count = (mesh.shape[axis] for axis in ("gr", "sp", "tp"))
    sp_axes = "sp"
    halves_mesh = mesh
    if sp_count % 2 == 0:
        halves_mesh = jax.sharding.Mesh(
            mesh.devices.reshape(groups, 2, sp_count // 2, tp_count), ("gr", "hi", "lo", "tp")
        )
        sp_axes = ("hi", "lo")

    def shards(tokens, norm_gain, w_key, w_value, new_query, cum_gate):
        seqs, positions, width = tokens.shape
        heads = w_key.shape[1] // HD
        alone = sp_count == seqs and tp_count == heads
        even = power_of_two(seqs) and power_of_two(heads) and positions % LANES == 0
        body = read_beside if alone and even and seqs // 2 == 2 else functools.partial(read_after, sp_axes)
        return body(tokens, norm_gain.reshape(1, width), w_key, w_value, new_query, cum_gate)

    sp = sp_axes if isinstance(sp_axes, tuple) else (sp_axes,)
    in_specs = (
        P("gr", sp + ("tp",), None),
        P(),
        P(),
        P(),
        P("gr", None, None),
        P(("gr",) + sp, "tp", None),
    )
    out_specs = (P(("gr",) + sp, "tp", None, None), P("gr", None, None))
    return jax.shard_map(
        shards, mesh=halves_mesh, in_specs=in_specs, out_specs=out_specs, check_vma=False
    )
```

```python
import functools

import jax
import jax.numpy as jnp
from jax import lax
from jax.experimental import pallas as pl
from jax.experimental.pallas import tpu as pltpu
from jax.sharding import PartitionSpec as P

HD = 64
LANES = 128
NORM_FLOOR = 0.05
F32 = jnp.float32
BF16 = jnp.bfloat16


def divisor_up_to(total, limit):
    size = min(total, limit)
    while total % size:
        size -= 1
    return size


def normalize(tokens, gain):
    widened = tokens.astype(F32)
    mean_square = jnp.mean(widened * widened, axis=-1, keepdims=True)
    return (widened * lax.rsqrt(mean_square + NORM_FLOOR) * gain).astype(BF16)


def keys_and_values(normed, key_ref, value_ref):
    keys = jnp.dot(normed, key_ref[...], preferred_element_type=F32)
    values = jnp.dot(normed, value_ref[...], preferred_element_type=F32)
    for head in range(key_ref.shape[1] // HD):
        columns = slice(head * HD, (head + 1) * HD)
        yield head, jnp.concatenate([keys[:, columns], values[:, columns]], axis=-1).astype(BF16)


def three_parts(value, axis=0):
    high = value.astype(BF16)
    rest = value - high.astype(F32)
    middle = rest.astype(BF16)
    low = (rest - middle.astype(F32)).astype(BF16)
    return jnp.concatenate([high, middle, low], axis=axis)


def project_kernel(tokens_ref, gain_ref, key_ref, value_ref, out_ref):
    normed = normalize(tokens_ref[0], gain_ref[...])
    for head, both in keys_and_values(normed, key_ref, value_ref):
        out_ref[0, head] = both


def project(tokens, norm_gain, w_key, w_value):
    seqs, positions, width = tokens.shape
    heads = w_key.shape[1] // HD
    tile = divisor_up_to(positions, 512)
    return pl.pallas_call(
        project_kernel,
        grid=(seqs, positions // tile),
        in_specs=[
            pl.BlockSpec((1, tile, width), lambda s, i: (s, i, 0)),
            pl.BlockSpec((1, width), lambda s, i: (0, 0)),
            pl.BlockSpec(w_key.shape, lambda s, i: (0, 0)),
            pl.BlockSpec(w_value.shape, lambda s, i: (0, 0)),
        ],
        out_specs=pl.BlockSpec((1, heads, tile, 2 * HD), lambda s, i: (s, 0, i, 0)),
        out_shape=jax.ShapeDtypeStruct((seqs, heads, positions, 2 * HD), BF16),
        name="project",
    )(tokens, norm_gain, w_key, w_value)


def softmax_part(query, block, gate):
    rows = query.shape[0]
    scores = lax.dot_general(query, block, (((1,), (1,)), ((), ())), preferred_element_type=F32)
    scores = scores * HD ** (-0.5) - gate
    top = jnp.max(scores, axis=1, keepdims=True)
    weights = jnp.exp(scores - top)
    parts = jnp.dot(three_parts(weights), block, preferred_element_type=F32)
    summed = parts[:rows] + parts[rows : 2 * rows] + parts[2 * rows :]
    return summed, top, jnp.sum(weights, axis=1, keepdims=True)


def packed(summed, top, total):
    lane = lax.broadcasted_iota(jnp.int32, summed.shape, summed.ndim - 1)
    return jnp.where(lane >= HD, summed, jnp.where(lane == 0, top, total))


def merged(tiles):
    best = functools.reduce(jnp.maximum, [tile[..., :1] for tile in tiles])
    factors = [jnp.exp(tile[..., :1] - best) for tile in tiles]
    both = sum(tile * factor for tile, factor in zip(tiles, factors))
    return both, best


def read_kernel(chunks, query_ref, cache_ref, gate_ref, out_ref):
    size = cache_ref.shape[0] // chunks
    tiles = []
    for c in range(chunks):
        rows = slice(c * size, (c + 1) * size)
        tiles.append(packed(*softmax_part(query_ref[...], cache_ref[rows, :], gate_ref[:, rows])))
    both, best = merged(tiles)
    out_ref[...] = packed(both, best, both[:, 1:2])


def read(queries, cache, gates):
    padded = jnp.concatenate([queries, jnp.zeros_like(queries)], axis=-1)
    chunks = 4
    while cache.shape[0] % chunks:
        chunks -= 1
    return pl.pallas_call(
        functools.partial(read_kernel, chunks),
        out_shape=jax.ShapeDtypeStruct((queries.shape[0], 2 * HD), F32),
        name="read",
    )(padded, cache, gates)


def read_after(sp_axes, tokens, norm_gain, w_key, w_value, new_query, cum_gate):
    seqs, positions, _ = tokens.shape
    sp_count, tp_count = lax.axis_size(sp_axes), lax.axis_size("tp")
    everyone = (sp_axes if isinstance(sp_axes, tuple) else (sp_axes,)) + ("tp",)
    heads = w_key.shape[1] // HD
    classes, halves = sp_count // seqs, tp_count // heads
    piece = positions // (classes * halves)
    devices = sp_count * tp_count
    made = project(tokens, norm_gain, w_key, w_value)
    made = made.reshape(seqs, heads, classes, halves, piece, 2 * HD).transpose(0, 2, 1, 3, 4, 5)
    arrived = lax.all_to_all(
        made.reshape(devices, piece, 2 * HD), everyone, split_axis=0, concat_axis=0, tiled=True
    )
    kv_cache = arrived.reshape(devices * piece, 2 * HD)
    query_heads = new_query.shape[1]
    group = query_heads // heads
    seq_index = lax.axis_index(sp_axes) // classes
    head_index = lax.axis_index("tp") // halves
    queries = lax.dynamic_slice(new_query, (seq_index, head_index * group, 0), (1, group, HD))[0]
    tile = read(queries, kv_cache, cum_gate[0])
    tiles = lax.all_gather(tile, everyone)
    tiles = tiles.reshape(seqs, classes, heads, halves, group, 2 * HD)
    tops = tiles[..., :1]
    factors = jnp.exp(tops - jnp.max(tops, axis=(1, 3), keepdims=True))
    both = jnp.sum(tiles * factors, axis=(1, 3))
    first_read = both[..., HD:] / both[..., 1:2]
    return kv_cache[None, None], first_read.reshape(seqs, query_heads, HD)


def heads_made(normed, key_ref, value_ref):
    return [both for _, both in keys_and_values(normed, key_ref, value_ref)]


def across_kernel(axes, flip, tokens_ref, gain_ref, key_hbm, value_hbm, *refs):
    heads = len(refs) - 5
    out_refs, (token_ref, weight_ref, made_ref, loads, stores) = refs[:heads], refs[heads:]
    upper, lower, column = (lax.axis_index(axis) for axis in axes)
    seq = (upper * lax.axis_size(axes[1]) + lower) ^ flip
    pieces, rows = token_ref.shape[:2]
    moves = [(tokens_ref.at[seq, pl.ds(i * rows, rows)], token_ref.at[i]) for i in range(pieces)]
    wide = key_hbm.shape[1]
    moves += [(key_hbm, weight_ref.at[:, pl.ds(0, wide)]), (value_hbm, weight_ref.at[:, pl.ds(wide, wide)])]
    copies = [
        pltpu.make_async_copy(source, target, loads.at[i]) for i, (source, target) in enumerate(moves)
    ]
    for copy in copies:
        copy.start()
    normed = []
    for i in range(pieces):
        copies[i].wait()
        normed.append(normalize(token_ref[i], gain_ref[...]))
    copies[pieces].wait()
    copies[pieces + 1].wait()
    writes = []
    for i in range(pieces):
        made = jnp.dot(normed[i], weight_ref[...], preferred_element_type=F32)
        part = slice(i * rows, (i + 1) * rows)
        for head in range(heads):
            k = made[:, head * HD : (head + 1) * HD]
            v = made[:, wide + head * HD : wide + (head + 1) * HD]
            made_ref[head, part] = jnp.concatenate([k, v], axis=-1).astype(BF16)
        for j, out_ref in enumerate(out_refs):
            source = made_ref.at[column ^ j, pl.ds(i * rows, rows)]
            target = out_ref.at[pl.ds(i * rows, rows)]
            writes.append(pltpu.make_async_copy(source, target, stores.at[i, j]))
            writes[-1].start()
    for write in writes:
        write.wait()


def make_across(axes, flip, tokens, norm_gain, w_key, w_value):
    _, positions, width = tokens.shape
    heads = w_key.shape[1] // HD
    pieces = 2
    anywhere, vmem = pl.BlockSpec(memory_space=pl.ANY), pl.BlockSpec(memory_space=pltpu.VMEM)
    return pl.pallas_call(
        functools.partial(across_kernel, axes, flip),
        in_specs=[anywhere, vmem, anywhere, anywhere],
        out_specs=[anywhere] * heads,
        out_shape=[jax.ShapeDtypeStruct((positions, 2 * HD), BF16)] * heads,
        scratch_shapes=[
            pltpu.VMEM((pieces, positions // pieces, width), BF16),
            pltpu.VMEM((width, 2 * w_key.shape[1]), BF16),
            pltpu.VMEM((heads, positions, 2 * HD), BF16),
            pltpu.SemaphoreType.DMA((pieces + 2,)),
            pltpu.SemaphoreType.DMA((pieces, heads)),
        ],
        name="across",
    )(tokens, norm_gain, w_key, w_value)


def planes(axes):
    upper, lower, column = (lax.axis_index(axis) for axis in axes)
    half = lax.axis_size(axes[1])
    return upper * half + lower, upper * half, column, half


def read_sequence(slots, blocks, query_ref, gate_ref, tile_ref):
    heads, group = len(blocks), query_ref.shape[1]
    lanes, queries, gates = 2 * HD, [], []
    for head, slot in enumerate(slots):
        query = query_ref[slot].astype(F32)
        pieces = [jnp.zeros((group, size), F32) for size in (head * lanes, (heads - head) * lanes - HD)]
        pieces.insert(1, query)
        queries.append(jnp.concatenate([piece for piece in pieces if piece.shape[1]], axis=1))
        lines = gate_ref[slot]
        gate = jnp.concatenate([lines[i : i + 1] for i in range(lines.shape[0])], axis=1)
        gates.append(jnp.broadcast_to(gate, (group, gate.shape[1])))
    query = jnp.concatenate(queries, axis=0).astype(BF16)
    block = jnp.concatenate(blocks, axis=1)
    summed, top, total = softmax_part(query, block, jnp.concatenate(gates, axis=0))
    for head, slot in enumerate(slots):
        rows = slice(head * group, (head + 1) * group)
        columns = slice(head * lanes, (head + 1) * lanes)
        tile_ref[slot] = packed(summed[rows, columns], top[rows], total[rows])


def rest_kernel(axes, heads, tokens_ref, gain_ref, key_ref, value_ref, query_ref, gate_ref, *refs):
    first_refs, refs = refs[:heads], refs[heads:]
    second_refs, (near_ref, tile_ref, _, made_ref, first_ref, loads) = refs[:heads], refs[heads:]
    step = pl.program_id(0)
    plane, near_first, column, half = planes(axes)
    copies = [
        pltpu.make_async_copy(source, first_ref.at[j], loads.at[j])
        for j, source in enumerate(first_refs)
    ]

    @pl.when(step == 0)
    def _():
        for copy in copies:
            copy.start()

    made = heads_made(normalize(tokens_ref[0], gain_ref[...]), key_ref, value_ref)
    seq = jnp.where(step == 0, plane ^ (half + 1), near_first + step - 1)
    slots = [seq * heads + head for head in range(heads)]
    read_sequence(slots, made, query_ref, gate_ref, tile_ref)

    @pl.when(step == 0)
    def _():
        for head, both in enumerate(made):
            made_ref[head] = both
        for j in range(heads):
            second_refs[j][...] = made_ref[column ^ j]

    @pl.when(step == pl.num_programs(0) - 1)
    def _():
        for copy in copies:
            copy.wait()
        slots = [(plane ^ half) * heads + (column ^ j) for j in range(heads)]
        read_sequence(slots, [first_ref[j] for j in range(heads)], query_ref, gate_ref, tile_ref)

    @pl.when(step > 0)
    def _():
        for head, both in enumerate(made):
            near_ref[0, head] = both


def make_rest(axes, tokens, norm_gain, w_key, w_value, queries, gates, first):
    seqs, positions, width = tokens.shape
    heads = w_key.shape[1] // HD
    near = seqs // 2
    fixed = lambda rank: lambda i: (0,) * rank
    tile_shape = queries.shape[:2] + (2 * HD,)

    def sequence(i):
        plane, near_first, _, half = planes(axes)
        return jnp.where(i == 0, plane ^ (half + 1), near_first + i - 1), 0, 0

    made = pl.pallas_call(
        functools.partial(rest_kernel, axes, heads),
        grid=(near + 1,),
        in_specs=[
            pl.BlockSpec((1, positions, width), sequence),
            pl.BlockSpec((1, width), fixed(2)),
            pl.BlockSpec(w_key.shape, fixed(2)),
            pl.BlockSpec(w_value.shape, fixed(2)),
            pl.BlockSpec(queries.shape, fixed(3)),
            pl.BlockSpec(gates.shape, fixed(3)),
        ]
        + [pl.BlockSpec(memory_space=pl.ANY)] * heads,
        out_specs=[pl.BlockSpec((positions, 2 * HD), fixed(2))] * heads
        + [
            pl.BlockSpec((1, heads, positions, 2 * HD), lambda i: (jnp.maximum(i - 1, 0), 0, 0, 0)),
            pl.BlockSpec(tile_shape, fixed(3)),
            pl.BlockSpec(memory_space=pl.ANY),
        ],
        scratch_shapes=[
            pltpu.VMEM((heads, positions, 2 * HD), BF16),
            pltpu.VMEM((heads, positions, 2 * HD), BF16),
            pltpu.SemaphoreType.DMA((heads,)),
        ],
        out_shape=[jax.ShapeDtypeStruct((positions, 2 * HD), BF16)] * heads
        + [
            jax.ShapeDtypeStruct((near, heads, positions, 2 * HD), BF16),
            jax.ShapeDtypeStruct(tile_shape, F32),
            jax.ShapeDtypeStruct((seqs * heads * positions, 2 * HD), BF16),
        ],
        name="rest",
    )(tokens, norm_gain, w_key, w_value, queries, gates, *first)
    return made[:heads], *made[heads:]


def merge(tiles):
    both, best = merged(tiles)
    return packed(both, best, both[..., 1:2])


def after(value, *others):
    return lax.optimization_barrier((value,) + others)[0]


def read_beside(tokens, norm_gain, w_key, w_value, new_query, cum_gate):
    seqs, positions, _ = tokens.shape
    heads = w_key.shape[1] // HD
    query_heads = new_query.shape[1]
    group = query_heads // heads
    devices = seqs * heads
    half = seqs // 2
    everyone = ("hi", "lo", "tp")
    plane = lax.axis_index("hi") * half + lax.axis_index("lo")
    column = lax.axis_index("tp")
    near_first = lax.axis_index("hi") * half
    weights = (norm_gain, w_key, w_value)

    def swap(value, k, j):
        pairs = [(i, i ^ (k * heads + j)) for i in range(devices)]
        return lax.ppermute(value, everyone, pairs)

    first = make_across(everyone, half, tokens, *weights)
    gates = after(cum_gate.reshape(devices, positions // LANES, LANES), first[0])
    gates = lax.all_to_all(gates, everyone, split_axis=0, concat_axis=0, tiled=True)
    ready, gates = lax.optimization_barrier((first[3], gates))
    blocks = [ready if j == 3 else block for j, block in enumerate(first)]
    arrived_first = [swap(block, half, j) for j, block in enumerate(blocks)]
    queries = new_query.reshape(devices, group, HD)
    rest = make_rest(everyone, tokens, *weights, queries, gates, first)
    second, near, tile, cache = rest
    arrived_second = [swap(second[j], half + 1, j) for j in range(heads)]
    near = near.reshape(half * heads, positions, 2 * HD)
    arrived_near = lax.all_to_all(near, ("lo", "tp"), split_axis=0, concat_axis=0, tiled=True)
    rows = devices * positions

    def placed(cache, blocks, k):
        for bit in range(heads.bit_length() - 1):
            swapped = ((column >> bit) & 1) == 1
            blocks = [
                jnp.where(swapped, blocks[head ^ (1 << bit)], block)
                for head, block in enumerate(blocks)
            ]
        start = (plane ^ k) * heads * positions
        return lax.dynamic_update_slice(cache, jnp.concatenate(blocks), (start, 0))

    def placed_alone(cache, block, k, j):
        start = ((plane ^ k) * heads + (column ^ j)) * positions
        return lax.dynamic_update_slice(cache, block, (start, 0))

    columns = [1 << bit for bit in reversed(range(1, heads.bit_length() - 1))]
    for j in columns:
        tile = merge([tile, swap(tile, 0, j)])
    odd = (column & 1) == 1
    low, high = tile[: devices // 2], tile[devices // 2 :]
    tile = jnp.where(odd, high, low)
    tile = merge([tile, swap(jnp.where(odd, low, high), 0, 1)])
    others = [swap(tile, k, 0) for k in range(1, seqs)]
    cache = placed(cache, arrived_first, half)
    for j, block in enumerate(arrived_second[:-1]):
        cache = placed_alone(cache, block, half + 1, j)
    near_rows = arrived_near.reshape(half * heads * positions, 2 * HD)
    cache = lax.dynamic_update_slice(cache, near_rows, (near_first * heads * positions, 0))
    tile = merge([tile] + others)
    tile = tile / tile[..., 1:2]
    other = swap(tile, 0, 1)
    pair = [jnp.where(odd, other, tile), jnp.where(odd, tile, other)]
    first_read = jnp.concatenate(pair)[..., HD:]
    cache = placed_alone(cache, arrived_second[-1], half + 1, heads - 1)
    return cache.reshape(1, 1, rows, 2 * HD), first_read.reshape(seqs, query_heads, HD)


def power_of_two(size):
    return size > 1 and size & (size - 1) == 0


def solution(mesh):
    groups, sp_count, tp_count = (mesh.shape[axis] for axis in ("gr", "sp", "tp"))
    sp_axes = "sp"
    halves_mesh = mesh
    if sp_count % 2 == 0:
        halves_mesh = jax.sharding.Mesh(
            mesh.devices.reshape(groups, 2, sp_count // 2, tp_count), ("gr", "hi", "lo", "tp")
        )
        sp_axes = ("hi", "lo")

    def shards(tokens, norm_gain, w_key, w_value, new_query, cum_gate):
        seqs, positions, width = tokens.shape
        heads = w_key.shape[1] // HD
        alone = sp_count == seqs and tp_count == heads
        even = power_of_two(seqs) and power_of_two(heads) and positions % LANES == 0
        body = read_beside if alone and even and seqs // 2 == 2 else functools.partial(read_after, sp_axes)
        return body(tokens, norm_gain.reshape(1, width), w_key, w_value, new_query, cum_gate)

    sp = sp_axes if isinstance(sp_axes, tuple) else (sp_axes,)
    in_specs = (
        P("gr", sp + ("tp",), None),
        P(),
        P(),
        P(),
        P("gr", None, None),
        P(("gr",) + sp, "tp", None),
    )
    out_specs = (P(("gr",) + sp, "tp", None, None), P("gr", None, None))
    return jax.shard_map(
        shards, mesh=halves_mesh, in_specs=in_specs, out_specs=out_specs, check_vma=False
    )
```
